32 devices in a mesh: grp: 2 (over y), fs: 4 (over z), tp: 4 (over x, core).
Axes of the slice: x: 2, y: 2, z: 4, core: 2. Of those that a mesh axis runs over, the one named last changes fastest.
Arguments:
- prompt: bfloat16 [2048, 2048], P(('grp', 'tp')), parts along dimension 0, may hold values from -6 to 6
- gain_first: float32 [2048], P('fs'), may hold values from 0.1 to 1.9
- gate_first: float32 [2048, 4096], P('fs', 'tp'), may hold values from -0.125 to 0.125
- up_first: float32 [2048, 4096], P('fs', 'tp'), may hold values from -0.125 to 0.125
- down_first: float32 [4096, 2048], P('fs', 'tp'), may hold values from -0.09375 to 0.09375
- gain_second: float32 [2048], P('fs'), may hold values from 0.1 to 1.9
- gate_second: float32 [2048, 4096], P('fs', 'tp'), may hold values from -0.125 to 0.125
- up_second: float32 [2048, 4096], P('fs', 'tp'), may hold values from -0.125 to 0.125
- down_second: float32 [4096, 2048], P('fs', 'tp'), may hold values from -0.09375 to 0.09375
Outputs:
- result: bfloat16 [2048, 2048], P(('grp', 'tp')), parts along dimension 0
- served_gate_first: bfloat16 [4096, 4096], P('grp', 'fs'), parts along dimension 0
- served_up_first: bfloat16 [4096, 4096], P('grp', 'fs'), parts along dimension 0
- served_down_first: bfloat16 [4096, 4096], P('fs', 'grp'), parts along dimension 1
- served_gate_second: bfloat16 [4096, 4096], P('grp', 'fs'), parts along dimension 0
- served_up_second: bfloat16 [4096, 4096], P('grp', 'fs'), parts along dimension 0
- served_down_second: bfloat16 [4096, 4096], P('fs', 'grp'), parts along dimension 1
The draws below stay inside these ranges and needn't reach their ends.
There are 2 independent parts, one for each index of `grp`. The reference program is written for one: setup_inputs(seed, part) draws one part's arguments, and reference() takes and returns one part's arrays. A program takes and returns all parts, laid end to end along the dimension named above; an argument that names none is the same for every part. Nothing has to cross between parts.
All inputs are finite; a program needn't handle non-finite values.
Results may differ from the reference program's by a relative error of at most 0.0053.
Values may be sent and summed in bfloat16 or wider, within the bound.
A program may use at most 128 MiB of HBM per device.

```python
import jax
import jax.numpy as jnp
from jax import lax

D = 2048
FF = 4096
TOKENS = 1024


def block_scale(rng, extent, shards, low, top_value):
    factor_of, own = 1.0, jax.random.fold_in(rng, 6)
    for position, blocks in shards:
        draws = jnp.exp(jax.random.uniform(jax.random.fold_in(own, position), (blocks,), jnp.float32, low / len(shards), top_value / len(shards)))
        factor_of = factor_of * jnp.repeat(draws, extent[position] // blocks).reshape([-1 if axis == position else 1 for axis in range(len(extent))])
    return factor_of


def gaussian(stream_key, dims, deviation, most, pieces=(), dtype=jnp.bfloat16):
    entries = deviation * jax.random.normal(stream_key, dims, jnp.float32)
    if pieces:
        entries = entries * block_scale(stream_key, dims, pieces, -0.22, 0.18)
    return jnp.clip(entries, -most, most).astype(dtype)


def setup_inputs(seed: int = 0, part: int = 0) -> dict:
    splits = jax.random.split(jax.random.key(seed), 10)
    own_keys = jax.random.split(jax.random.fold_in(splits[9], part), 10)
    return {
        "prompt": gaussian(own_keys[0], (TOKENS, D), 1.0, 6.0, ((0, 4),)),
        "gain_first": jnp.clip(1.0 + 0.18 * jax.random.normal(splits[1], (D,), jnp.float32), 0.1, 1.9),
        "gate_first": gaussian(splits[2], (D, FF), D ** -0.5, 0.125, ((0, 4), (1, 4)), jnp.float32),
        "up_first": gaussian(splits[3], (D, FF), D ** -0.5, 0.125, ((0, 4), (1, 4)), jnp.float32),
        "down_first": gaussian(splits[4], (FF, D), FF ** -0.5, 0.09375, ((0, 4), (1, 4)), jnp.float32),
        "gain_second": jnp.clip(1.0 + 0.18 * jax.random.normal(splits[5], (D,), jnp.float32), 0.1, 1.9),
        "gate_second": gaussian(splits[6], (D, FF), D ** -0.5, 0.125, ((0, 4), (1, 4)), jnp.float32),
        "up_second": gaussian(splits[7], (D, FF), D ** -0.5, 0.125, ((0, 4), (1, 4)), jnp.float32),
        "down_second": gaussian(splits[8], (FF, D), FF ** -0.5, 0.09375, ((0, 4), (1, 4)), jnp.float32),
    }


EPS = 1e-06

def fold(gain, weight):
    return (gain[:, None] * weight).astype(jnp.bfloat16)

def normed_of(stream):
    return (stream * lax.rsqrt(lax.optimization_barrier(jnp.mean(stream * stream, axis=-1, keepdims=True)) + EPS)).astype(jnp.bfloat16)

def block(stream, w_gate, w_up, w_down):
    normed = normed_of(stream)
    gate = jnp.dot(normed, w_gate, preferred_element_type=jnp.float32)
    up_val = jnp.dot(normed, w_up, preferred_element_type=jnp.float32)
    hidden = (jax.nn.silu(gate) * up_val).astype(jnp.bfloat16)
    return stream + 0.5 * jnp.dot(hidden, w_down, preferred_element_type=jnp.float32)

def reference(prompt, gain_first, gate_first, up_first, down_first, gain_second, gate_second, up_second, down_second):
    g_one = fold(gain_first, gate_first)
    u_one = fold(gain_first, up_first)
    d_one = down_first.astype(jnp.bfloat16)
    g_two = fold(gain_second, gate_second)
    u_two = fold(gain_second, up_second)
    d_two = down_second.astype(jnp.bfloat16)
    stream = prompt.astype(jnp.float32)
    stream = block(stream, g_one, u_one, d_one)
    stream = block(stream, g_two, u_two, d_two)
    return (stream.astype(jnp.bfloat16), g_one, u_one, d_one, g_two, u_two, d_two)
```

```python
import functools

import jax
import jax.numpy as jnp
from jax import lax
from jax.experimental import pallas as pl
from jax.experimental.pallas import tpu as pltpu
from jax.sharding import PartitionSpec as P

EPS = 1e-06
MESH = pl.DeviceIdType.MESH
LANES = 128
LAG = 2


def kernel(n_grp, n_fs, n_tp, n_sub, *refs):
    prompt, gains, weights, downs = refs[0], refs[1:3], refs[3:7], refs[7:9]
    result, served, served_down = refs[9], refs[10:14], refs[14:16]
    (land, own, scale, stream, normed, hidden, onward, inward, middle, delta, stage) = refs[16:27]
    (load_sem, prompt_sem,
     p_send, p_recv, r_send, z_send, z_recv, x_send, x_recv, y_send, y_recv, c_send, c_recv, own_sem,
     dx_send, dx_recv, dy_send, dy_recv, dc_send, dc_recv,
     s_send, u_recv, m_recv, o_send, o_recv) = refs[27:]

    g, f, t = lax.axis_index("grp"), lax.axis_index("fs"), lax.axis_index("tp")
    ratio = n_fs // n_tp
    chips = n_tp // 2
    home = f // ratio
    mine_sub = lax.rem(t + n_tp - home, n_tp) // 2
    carries = mine_sub < n_sub
    is_lane = lax.rem(t, 2) == lax.rem(home, 2)
    partner = t + 1 - 2 * lax.rem(t, 2)

    half = n_fs // 2
    lower = f < half
    is_mid = jnp.logical_or(f == half - 1, f == half)
    is_end = jnp.logical_or(f == 0, f == n_fs - 1)
    toward = jnp.where(lower, f + 1, f - 1)
    away = jnp.where(lower, jnp.maximum(f - 1, 0), jnp.minimum(f + 1, n_fs - 1))

    def along_fs(o):
        return lax.rem(f + o, n_fs)

    def along_tp(dx):
        return lax.rem(t + 2 * dx, n_tp)

    def along_grp(dg):
        return lax.rem(g + dg, n_grp)

    def remote(src, dst, send, recv, where):
        return pltpu.make_async_remote_copy(
            src_ref=src, dst_ref=dst, send_sem=send, recv_sem=recv,
            device_id=where, device_id_type=MESH,
        )

    def arrived(dst, sem):
        pltpu.make_async_copy(dst, dst, sem).wait()

    rows, columns = weights[0].shape
    share = rows // n_grp
    sub = share // n_sub
    width = served[0].shape[1]
    d_rows, d_cols = downs[0].shape
    d_share = d_rows // n_grp
    tokens, features = prompt.shape
    slab = min(64, tokens)
    tile = min(256, width)
    wide = min(256, features)
    chunks = features // wide

    def landing(n):
        return land[n % 3] if n < 4 else land[3]

    def load(n):
        src = weights[n] if n < 4 else downs[n - 4]
        return pltpu.make_async_copy(src, landing(n), load_sem.at[n])

    def spread_gain(k):
        gain = gains[k]
        if gain.shape[0] == rows:
            scale[k] = gain[...]
        else:
            scale[k] = jnp.broadcast_to(gain[...], (LANES, rows)).T

    def fold(m):
        load(m).wait()
        step = min(64, rows)

        @pl.loop(0, rows // step)
        def _(i):
            at = pl.ds(pl.multiple_of(i * step, step), step)
            factor = scale[m // 2, at]
            for j in range(columns // LANES):
                lanes = pl.ds(j * LANES, LANES)
                own[m, at, lanes] = (factor * landing(m)[at, lanes]).astype(jnp.bfloat16)

    def round_down(k):
        load(4 + k).wait()
        step = min(64, d_rows)

        @pl.loop(0, d_rows // step)
        def _(i):
            at = pl.ds(pl.multiple_of(i * step, step), step)
            to = pl.ds(pl.multiple_of(t * d_cols, d_cols), d_cols)
            served_down[k][at, to] = landing(4 + k)[at].astype(jnp.bfloat16)

    def piece(m, r, h, s):
        return served[m].at[pl.ds(pl.multiple_of(r * rows + h * share + s * sub, sub), sub)]

    def p_copy(m, s):
        src = own.at[m, pl.ds(pl.multiple_of(g * share + s * sub, sub), sub)]
        return remote(src, stage.at[m, s - 1], p_send.at[m, s - 1], p_recv.at[m, s - 1], {"tp": along_tp(s)})

    def p_start(m):
        for s in range(1, n_sub):
            p_copy(m, s).start()

    def z_copy(m, s, j):
        cut = pl.ds(j * width, width)
        if s == 0:
            src = own.at[m, pl.ds(pl.multiple_of(g * share, share), sub), cut]
            return src, piece(m, f, g, s), t * ratio + j
        source = lax.rem(t + n_tp - 2 * s, n_tp)
        return stage.at[m, s - 1, :, cut], piece(m, f, g, s), source * ratio + j

    def z_remote(m, s, j):
        src, dst, to = z_copy(m, s, j)
        send = z_send.at[m, j] if s == 0 else r_send.at[m, s - 1, j]
        return remote(src, dst, send, z_recv.at[m, f], {"fs": to})

    def z_start(m, s):
        for j in range(ratio):
            src, dst, to = z_copy(m, s, j)

            @pl.when(to != f)
            def _():
                z_remote(m, s, j).start()

            @pl.when(to == f)
            def _():
                pltpu.make_async_copy(src, dst, own_sem.at[m]).start()

    def relay(m):
        for s in range(1, n_sub):
            arrived(stage.at[m, s - 1], p_recv.at[m, s - 1])
            z_start(m, s)

    def x_copy(m, r, dx):
        ref = piece(m, r, g, mine_sub)
        return remote(ref, ref, x_send.at[m, r, dx - 1], x_recv.at[m, r, mine_sub], {"tp": along_tp(dx)})

    def y_copy(m, r, dg, s):
        ref = piece(m, r, g, s)
        return remote(ref, ref, y_send.at[m, r, dg - 1, s], y_recv.at[m, r, g, s], {"grp": along_grp(dg)})

    def c_copy(m, r, h, s):
        ref = piece(m, r, h, s)
        return remote(ref, ref, c_send.at[m, r, h, s], c_recv.at[m, r, h, s], {"tp": partner})

    def primary(m):
        @pl.when(is_lane)
        def _():
            @pl.loop(0, n_fs)
            def _(o):
                r = along_fs(o)

                @pl.when(carries)
                def _():
                    @pl.when(o == 0)
                    def _():
                        arrived(piece(m, r, g, mine_sub), own_sem.at[m])

                    @pl.when(o != 0)
                    def _():
                        arrived(piece(m, r, g, mine_sub), z_recv.at[m, r])

                    for dx in range(1, chips):
                        x_copy(m, r, dx).start()
                    for dg in range(1, n_grp):
                        y_copy(m, r, dg, mine_sub).start()
                    c_copy(m, r, g, mine_sub).start()

    def crossed_step(m, o):
        r = along_fs(o)
        for s in range(n_sub):
            @pl.when(mine_sub != s)
            def _():
                arrived(piece(m, r, g, s), x_recv.at[m, r, s])
                for dg in range(1, n_grp):
                    y_copy(m, r, dg, s).start()
                c_copy(m, r, g, s).start()

    def crossed(m):
        @pl.when(is_lane)
        def _():
            @pl.loop(0, n_fs)
            def _(o):
                crossed_step(m, o)

    def secondary(m):
        @pl.when(is_lane)
        def _():
            @pl.loop(0, n_fs)
            def _(o):
                r = along_fs(o)
                for dg in range(1, n_grp):
                    h = along_grp(dg)
                    for s in range(n_sub):
                        arrived(piece(m, r, h, s), y_recv.at[m, r, h, s])
                        c_copy(m, r, h, s).start()

    def complete(m):
        @pl.when(jnp.logical_not(is_lane))
        def _():
            @pl.loop(0, n_fs)
            def _(r):
                for h in range(n_grp):
                    for s in range(n_sub):
                        arrived(piece(m, r, h, s), c_recv.at[m, r, h, s])

    direct = (True, False)

    def d_piece(k, s, h):
        return served_down[k].at[
            pl.ds(pl.multiple_of(h * d_share, d_share), d_share),
            pl.ds(pl.multiple_of(s * d_cols, d_cols), d_cols),
        ]

    def d_block(k, s):
        return served_down[k].at[:, pl.ds(pl.multiple_of(s * d_cols, d_cols), d_cols)]

    def d_first(k, s):
        return d_block(k, s) if direct[k] else d_piece(k, s, g)

    def dx_copy(k, dx):
        ref = d_first(k, t)
        return remote(ref, ref, dx_send.at[k, dx - 1], dx_recv.at[k, dx - 1], {"tp": along_tp(dx)})

    def dy_copy(k, dx, dg):
        ref = d_piece(k, lax.rem(t + n_tp - 2 * dx, n_tp), g)
        return remote(ref, ref, dy_send.at[k, dx - 1, dg - 1], dy_recv.at[k, dx - 1, dg - 1], {"grp": along_grp(dg)})

    def dc_copy(k, dx):
        ref = d_block(k, lax.rem(t + n_tp - 2 * dx, n_tp))
        return remote(ref, ref, dc_send.at[k, dx], dc_recv.at[k, dx], {"tp": partner})

    def down_start(k):
        for dx in range(1, chips):
            dx_copy(k, dx).start()
        dc_copy(k, 0).start()

    def down_primary(k):
        if direct[k]:
            return
        for dx in range(1, chips):
            source = lax.rem(t + n_tp - 2 * dx, n_tp)
            arrived(d_piece(k, source, g), dx_recv.at[k, dx - 1])
            for dg in range(1, n_grp):
                dy_copy(k, dx, dg).start()

    def down_secondary(k):
        for dx in range(1, chips):
            source = lax.rem(t + n_tp - 2 * dx, n_tp)
            if direct[k]:
                arrived(d_block(k, source), dx_recv.at[k, dx - 1])
            else:
                for dg in range(1, n_grp):
                    arrived(d_piece(k, source, lax.rem(g + n_grp - dg, n_grp)), dy_recv.at[k, dx - 1, dg - 1])
            dc_copy(k, dx).start()
        for dx in range(chips):
            arrived(d_block(k, lax.rem(partner + n_tp - 2 * dx, n_tp)), dc_recv.at[k, dx])

    final = (delta, result)

    def to_middle(k, i):
        return remote(onward.at[k, i], middle.at[k, i], s_send.at[k, i], m_recv.at[k, i], {"fs": toward})

    def to_next(k, i):
        return remote(onward.at[k, i], inward.at[k, i], s_send.at[k, i], u_recv.at[k, i], {"fs": toward})

    def to_outer(k, i):
        ref = final[k].at[i]
        return remote(ref, ref, o_send.at[k, i], o_recv.at[k, i], {"fs": away})

    def gather_in(k, i):
        at = pl.ds(pl.multiple_of(i * wide, wide), wide)
        value = jnp.dot(hidden[...], served_down[k][:, at], preferred_element_type=jnp.float32)

        @pl.when(is_end)
        def _():
            onward[k, i] = value.astype(jnp.bfloat16)

        @pl.when(jnp.logical_not(is_end))
        def _():
            arrived(inward.at[k, i], u_recv.at[k, i])
            onward[k, i] = (value + inward[k, i].astype(jnp.float32)).astype(jnp.bfloat16)

        @pl.when(is_mid)
        def _():
            to_middle(k, i).start()

        @pl.when(jnp.logical_not(is_mid))
        def _():
            to_next(k, i).start()

    def spread_out(k, i):
        at = pl.ds(pl.multiple_of(i * wide, wide), wide)

        @pl.when(is_mid)
        def _():
            arrived(middle.at[k, i], m_recv.at[k, i])
            total = 0.5 * (onward[k, i].astype(jnp.float32) + middle[k, i].astype(jnp.float32))
            if k == 1:
                total = stream[:, at] + total
            final[k][i] = total.astype(jnp.bfloat16)

        @pl.when(jnp.logical_not(is_mid))
        def _():
            arrived(final[k].at[i], o_recv.at[k, i])

        @pl.when(jnp.logical_not(is_end))
        def _():
            to_outer(k, i).start()

        if k == 0:
            stream[:, at] = stream[:, at] + delta[i].astype(jnp.float32)

    def reduce(k, beside=None):
        @pl.loop(0, chunks + LAG)
        def _(i):
            @pl.when(i < chunks)
            def _():
                gather_in(k, i)
                if beside is not None:
                    beside(i)

            @pl.when(i >= LAG)
            def _():
                spread_out(k, i - LAG)

    def norm():
        @pl.loop(0, tokens // slab)
        def _(i):
            at = pl.ds(pl.multiple_of(i * slab, slab), slab)
            value = stream[at]
            factor = lax.rsqrt(jnp.mean(value * value, axis=-1, keepdims=True) + EPS)
            normed[at] = (value * factor).astype(jnp.bfloat16)

    def multiply(k):
        w_gate, w_up = served[2 * k], served[2 * k + 1]

        @pl.loop(0, width // tile)
        def _(i):
            at = pl.ds(pl.multiple_of(i * tile, tile), tile)
            gate = jnp.dot(normed[...], w_gate[:, at], preferred_element_type=jnp.float32)
            up = jnp.dot(normed[...], w_up[:, at], preferred_element_type=jnp.float32)
            hidden[:, at] = (jax.nn.silu(gate) * up).astype(jnp.bfloat16)

    for n in (0, 1, 2, 4):
        load(n).start()
    prompt_copy = pltpu.make_async_copy(prompt, normed, prompt_sem)
    prompt_copy.start()

    barrier = pltpu.get_barrier_semaphore()
    peers = (
        [{"fs": along_fs(o)} for o in range(1, n_fs)]
        + [{"tp": along_tp(dx)} for dx in range(1, chips)]
        + [{"grp": along_grp(dg)} for dg in range(1, n_grp)]
        + [{"tp": partner}]
    )
    for peer in peers:
        pl.semaphore_signal(barrier, inc=1, device_id=peer, device_id_type=MESH)
    spread_gain(0)
    fold(0)
    pl.semaphore_wait(barrier, len(peers))

    p_start(0)
    z_start(0, 0)
    load(3).start()
    fold(1)
    p_start(1)
    z_start(1, 0)
    spread_gain(1)
    round_down(0)
    load(5).start()
    fold(2)
    fold(3)
    round_down(1)
    prompt_copy.wait()
    stream[...] = normed[...].astype(jnp.float32)
    norm()

    relay(0)
    relay(1)
    primary(0)
    p_start(2)
    z_start(2, 0)
    primary(1)
    p_start(3)
    z_start(3, 0)
    crossed(0)
    relay(2)
    down_start(0)
    crossed(1)
    relay(3)
    primary(2)
    primary(3)
    down_secondary(0)
    secondary(0)
    secondary(1)
    complete(0)
    complete(1)
    multiply(0)
    down_start(1)

    def beside(i):
        @pl.when(is_lane)
        def _():
            per = -(-2 * n_fs // chunks)
            for q in range(per):
                n = i * per + q

                @pl.when(n < n_fs)
                def _():
                    crossed_step(2, n)

                @pl.when(jnp.logical_and(n >= n_fs, n < 2 * n_fs))
                def _():
                    crossed_step(3, n - n_fs)

    reduce(0, beside)
    norm()
    down_primary(1)
    secondary(2)
    secondary(3)
    complete(2)
    complete(3)
    multiply(1)
    down_secondary(1)
    reduce(1)

    for m in range(4):
        for s in range(n_sub):
            if s > 0:
                p_copy(m, s).wait_send()
            for j in range(ratio):
                @pl.when(z_copy(m, s, j)[2] != f)
                def _():
                    z_remote(m, s, j).wait_send()

        @pl.when(is_lane)
        def _():
            @pl.loop(0, n_fs)
            def _(r):
                @pl.when(carries)
                def _():
                    for dx in range(1, chips):
                        x_copy(m, r, dx).wait_send()

                for s in range(n_sub):
                    for dg in range(1, n_grp):
                        y_copy(m, r, dg, s).wait_send()
                    for h in range(n_grp):
                        c_copy(m, r, h, s).wait_send()

    for k in range(2):
        dc_copy(k, 0).wait_send()
        for dx in range(1, chips):
            dx_copy(k, dx).wait_send()
            dc_copy(k, dx).wait_send()
            if not direct[k]:
                for dg in range(1, n_grp):
                    dy_copy(k, dx, dg).wait_send()

        @pl.loop(0, chunks)
        def _(i):
            @pl.when(is_mid)
            def _():
                to_middle(k, i).wait_send()

            @pl.when(jnp.logical_not(is_mid))
            def _():
                to_next(k, i).wait_send()

            @pl.when(jnp.logical_not(is_end))
            def _():
                to_outer(k, i).wait_send()


def store(parts, *refs):
    ins, outs, sems = refs[:7], refs[7:14], refs[14]
    copies = []
    chunks, _, wide = ins[0].shape
    for i in range(chunks):
        copies.append((ins[0].at[i], outs[0].at[:, pl.ds(i * wide, wide)]))
    for src, dst in zip(ins[1:], outs[1:]):
        rows = src.shape[0] // parts
        for i in range(parts):
            at = pl.ds(i * rows, rows)
            copies.append((src.at[at], dst.at[at]))
    copies = [pltpu.make_async_copy(src, dst, sems.at[i]) for i, (src, dst) in enumerate(copies)]
    for copy in copies:
        copy.start()
    for copy in copies:
        copy.wait()


def on_device(
    n_grp, n_fs, n_tp,
    prompt,
    gain_first,
    gate_first,
    up_first,
    down_first,
    gain_second,
    gate_second,
    up_second,
    down_second,
):
    tokens, features = prompt.shape
    rows, columns = gate_first.shape
    width = columns * n_tp // n_fs
    d_rows, d_cols = down_first.shape
    chips = n_tp // 2
    wide = min(256, features)
    chunks = features // wide
    gate_shape, down_shape = (features, width), (d_rows, features)
    bf16 = functools.partial(jax.ShapeDtypeStruct, dtype=jnp.bfloat16)
    share = rows // n_grp
    n_sub = chips if share % (16 * chips) == 0 else 1
    other_x, other_g = max(chips - 1, 1), max(n_grp - 1, 1)
    sems = [
        (6,), (),
        (4, other_x), (4, other_x), (4, other_x, n_fs // n_tp),
        (4, n_fs // n_tp), (4, n_fs), (4, n_fs, other_x), (4, n_fs, n_sub), (4, n_fs, other_g, n_sub),
        (4, n_fs, n_grp, n_sub), (4, n_fs, n_grp, n_sub), (4, n_fs, n_grp, n_sub), (4,),
        (2, other_x), (2, other_x), (2, other_x, other_g), (2, other_x, other_g),
        (2, chips), (2, chips),
        (2, chunks), (2, chunks), (2, chunks), (2, chunks), (2, chunks),
    ]
    if rows % LANES == 0:
        gains = [gain.reshape(1, rows) for gain in (gain_first, gain_second)]
    else:
        gains = [jnp.broadcast_to(gain[:, None], (rows, LANES)) for gain in (gain_first, gain_second)]
    far = functools.partial(pltpu.with_memory_space_constraint, memory_space=pltpu.HBM)
    vmem, hbm = pl.BlockSpec(memory_space=pltpu.VMEM), pl.BlockSpec(memory_space=pltpu.HBM)
    shapes = [(chunks, tokens, wide)] + [gate_shape] * 4 + [down_shape] * 2
    held = pl.pallas_call(
        functools.partial(kernel, n_grp, n_fs, n_tp, n_sub),
        out_shape=[bf16(s) for s in shapes],
        in_specs=[hbm] + [vmem] * 2 + [hbm] * 6,
        out_specs=[vmem] * 7,
        scratch_shapes=[
            [pltpu.VMEM((rows, columns), jnp.float32)] * 3 + [pltpu.VMEM((d_rows, d_cols), jnp.float32)],
            pltpu.VMEM((4, rows, columns), jnp.bfloat16),
            pltpu.VMEM((2, rows, LANES), jnp.float32),
            pltpu.VMEM((tokens, features), jnp.float32),
            pltpu.VMEM((tokens, features), jnp.bfloat16),
            pltpu.VMEM((tokens, width), jnp.bfloat16),
            pltpu.VMEM((2, chunks, tokens, wide), jnp.bfloat16),
            pltpu.VMEM((2, chunks, tokens, wide), jnp.bfloat16),
            pltpu.VMEM((2, chunks, tokens, wide), jnp.bfloat16),
            pltpu.VMEM((chunks, tokens, wide), jnp.bfloat16),
            pltpu.VMEM((4, other_x, share // n_sub, columns), jnp.bfloat16),
        ]
        + [pltpu.SemaphoreType.DMA(s) for s in sems],
        compiler_params=pltpu.CompilerParams(
            collective_id=0, has_side_effects=True, vmem_limit_bytes=26 * 2**20
        ),
        name="serve",
    )(far(prompt), *gains, *map(far, (gate_first, up_first, gate_second, up_second, down_first, down_second)))
    parts = 4
    result, g1, u1, g2, u2, d1, d2 = pl.pallas_call(
        functools.partial(store, parts),
        out_shape=[bf16((tokens, features))] + [bf16(s) for s in shapes[1:]],
        in_specs=[vmem] * 7,
        out_specs=[hbm] * 7,
        scratch_shapes=[pltpu.SemaphoreType.DMA((chunks + 6 * parts,))],
        compiler_params=pltpu.CompilerParams(vmem_limit_bytes=2**20),
        name="store",
    )(*held)
    return (result, g1, u1, d1, g2, u2, d2)
def solution(mesh):
    return jax.shard_map(
        functools.partial(on_device, mesh.shape["grp"], mesh.shape["fs"], mesh.shape["tp"]),
        mesh=mesh,
        in_specs=(
            P(("grp", "tp"), None),
            P("fs"),
            P("fs", "tp"),
            P("fs", "tp"),
            P("fs", "tp"),
            P("fs"),
            P("fs", "tp"),
            P("fs", "tp"),
            P("fs", "tp"),
        ),
        out_specs=(
            P(("grp", "tp"), None),
            P("grp", "fs"),
            P("grp", "fs"),
            P("fs", "grp"),
            P("grp", "fs"),
            P("grp", "fs"),
            P("fs", "grp"),
        ),
        check_vma=False,
    )
```

```python
import functools

import jax
import jax.numpy as jnp
from jax import lax
from jax.experimental import pallas as pl
from jax.experimental.pallas import tpu as pltpu
from jax.sharding import PartitionSpec as P

EPS = 1e-06
MESH = pl.DeviceIdType.MESH
LANES = 128
LAG = 2
HALVES = 2
SPLIT = 4
WHOLE = (False, False, True, False)
DIRECT = (True, True)


def kernel(n_grp, n_fs, n_tp, n_sub, *refs):
    prompt, gains, weights, downs = refs[0], refs[1:3], refs[3:7], refs[7:9]
    result, served, served_down = refs[9], refs[10:14], refs[14:16]
    (land, own, scale, stream, normed, hidden, onward, inward, middle, delta, stage) = refs[16:27]
    (load_sem, prompt_sem,
     p_send, p_recv, r_send, z_send, z_recv, x_send, x_recv, y_send, y_recv, c_send, c_recv, own_sem,
     dx_send, dx_recv, dy_send, dy_recv, dc_send, dc_recv,
     s_send, u_recv, m_recv, o_send, o_recv) = refs[27:]

    g, f, t = lax.axis_index("grp"), lax.axis_index("fs"), lax.axis_index("tp")
    ratio = n_fs // n_tp
    chips = n_tp // 2
    home = f // ratio
    mine_sub = lax.rem(t // 2 + chips - home // 2, chips)
    carries = mine_sub < n_sub
    partner = t + 1 - 2 * lax.rem(t, 2)

    def lane(m):
        return lax.rem(t + m, 2) == lax.rem(home, 2)

    def other_lane(m):
        return lax.rem(t + m, 2) != lax.rem(home, 2)

    half = n_fs // 2
    lower = f < half
    is_mid = jnp.logical_or(f == half - 1, f == half)
    is_end = jnp.logical_or(f == 0, f == n_fs - 1)
    toward = jnp.where(lower, f + 1, f - 1)
    away = jnp.where(lower, jnp.maximum(f - 1, 0), jnp.minimum(f + 1, n_fs - 1))

    step = jnp.where(lower, 1, n_fs - 1)

    def along_fs(o):
        return lax.rem(f + o, n_fs)

    def by_way(o):
        return lax.rem(f + o * step, n_fs)

    def along_tp(dx):
        return lax.rem(t + 2 * dx, n_tp)

    def along_grp(dg):
        return lax.rem(g + dg, n_grp)

    def remote(src, dst, send, recv, where):
        return pltpu.make_async_remote_copy(
            src_ref=src, dst_ref=dst, send_sem=send, recv_sem=recv,
            device_id=where, device_id_type=MESH,
        )

    def arrived(dst, sem):
        pltpu.make_async_copy(dst, dst, sem).wait()

    rows, columns = weights[0].shape
    share = rows // n_grp
    subs = [1 if whole else n_sub for whole in WHOLE]
    columns_to = [chips if whole else n_sub for whole in WHOLE]
    width = served[0].shape[1]
    d_rows, d_cols = downs[0].shape
    d_share = d_rows // n_grp
    tokens, features = prompt.shape
    slab = min(64, tokens)
    tile = min(256, width)
    wide = min(256, features)
    chunks = features // wide
    halves, part_rows, _ = result.shape[0] // chunks, *result.shape[1:]

    def landing(n):
        return land[n % 3] if n < 4 else land[3]

    def load(n):
        src = weights[n] if n < 4 else downs[n - 4]
        return pltpu.make_async_copy(src, landing(n), load_sem.at[n])

    def spread_gain(k):
        gain = gains[k]
        if gain.shape[0] == rows:
            scale[k] = gain[...]
        else:
            scale[k] = jnp.broadcast_to(gain[...], (LANES, rows)).T

    def fold(m):
        load(m).wait()
        step = min(64, rows)

        @pl.loop(0, rows // step)
        def _(i):
            at = pl.ds(pl.multiple_of(i * step, step), step)
            factor = scale[m // 2, at]
            for j in range(columns // LANES):
                lanes = pl.ds(j * LANES, LANES)
                own[m, at, lanes] = (factor * landing(m)[at, lanes]).astype(jnp.bfloat16)

    def round_down(k):
        load(4 + k).wait()
        step = min(64, d_rows)

        @pl.loop(0, d_rows // step)
        def _(i):
            at = pl.ds(pl.multiple_of(i * step, step), step)
            to = pl.ds(pl.multiple_of(t * d_cols, d_cols), d_cols)
            served_down[k][at, to] = landing(4 + k)[at].astype(jnp.bfloat16)

    def carried(m, s):
        return 0 if WHOLE[m] else s

    def piece(m, r, h, s):
        sub = share // subs[m]
        return served[m].at[pl.ds(pl.multiple_of(r * rows + h * share + s * sub, sub), sub)]

    def own_rows(m, s):
        sub = share // subs[m]
        return pl.ds(pl.multiple_of(g * share + carried(m, s) * sub, sub), sub)

    def p_copy(m, s):
        src = own.at[m, own_rows(m, s)]
        return remote(src, stage[m].at[s - 1], p_send.at[m, s - 1], p_recv.at[m, s - 1], {"tp": along_tp(s)})

    def p_start(m):
        for s in range(1, columns_to[m]):
            p_copy(m, s).start()

    def z_copy(m, s, j):
        cut = pl.ds(j * width, width)
        if s == 0:
            return own.at[m, own_rows(m, 0), cut], piece(m, f, g, 0), t * ratio + j
        source = lax.rem(t + n_tp - 2 * s, n_tp)
        return stage[m].at[s - 1, :, cut], piece(m, f, g, carried(m, s)), source * ratio + j

    def z_remote(m, s, j):
        src, dst, to = z_copy(m, s, j)
        send = z_send.at[m, j] if s == 0 else r_send.at[m, s - 1, j]
        where = {"fs": to} if m % 2 == 0 else {"fs": to, "tp": partner}
        return remote(src, dst, send, z_recv.at[m, f], where)

    def z_aside(m, s, j):
        src, dst, _ = z_copy(m, s, j)
        send = z_send.at[m, j] if s == 0 else r_send.at[m, s - 1, j]
        return remote(src, dst, send, own_sem.at[m], {"tp": partner})

    def z_start(m, s):
        for j in range(ratio):
            src, dst, to = z_copy(m, s, j)

            @pl.when(to != f)
            def _():
                z_remote(m, s, j).start()

            @pl.when(to == f)
            def _():
                if m % 2 == 0:
                    pltpu.make_async_copy(src, dst, own_sem.at[m]).start()
                else:
                    z_aside(m, s, j).start()

    def relay(m):
        for s in range(1, columns_to[m]):
            arrived(stage[m].at[s - 1], p_recv.at[m, s - 1])
            z_start(m, s)

    def x_copy(m, r, dx):
        ref = piece(m, r, g, mine_sub)
        return remote(ref, ref, x_send.at[m, r, dx - 1], x_recv.at[m, r, mine_sub], {"tp": along_tp(dx)})

    def y_copy(m, r, dg, s):
        ref = piece(m, r, g, s)
        return remote(ref, ref, y_send.at[m, r, dg - 1, s], y_recv.at[m, r, g, s], {"grp": along_grp(dg)})

    def c_copy(m, r, h, s):
        ref = piece(m, r, h, s)
        return remote(ref, ref, c_send.at[m, r, h, s], c_recv.at[m, r, h, s], {"tp": partner})

    def primary_step(m, o):
        r = by_way(o)
        s = 0 if WHOLE[m] else mine_sub
        ref = piece(m, r, g, s)

        def onward_from(first):
            arrived(ref, own_sem.at[m] if first else z_recv.at[m, r])
            if not WHOLE[m]:
                for dx in range(1, chips):
                    x_copy(m, r, dx).start()
            for dg in range(1, n_grp):
                y_copy(m, r, dg, s).start()
            c_copy(m, r, g, s).start()

        if WHOLE[m]:
            onward_from(isinstance(o, int))
        else:
            @pl.when(carries)
            def _():
                onward_from(isinstance(o, int))

    def own_first(m):
        @pl.when(jnp.logical_and(lane(m), mine_sub == 0))
        def _():
            primary_step(m, 0)

    def own_later(m):
        @pl.when(jnp.logical_and(lane(m), mine_sub != 0))
        def _():
            primary_step(m, 0)

    def primary(m, low=1, high=n_fs):
        @pl.when(lane(m))
        def _():
            @pl.loop(low, high)
            def _(o):
                primary_step(m, o)

    def crossed_step(m, o):
        r = by_way(o)
        for s in range(0 if WHOLE[m] else n_sub):
            @pl.when(mine_sub != s)
            def _():
                arrived(piece(m, r, g, s), x_recv.at[m, r, s])
                for dg in range(1, n_grp):
                    y_copy(m, r, dg, s).start()
                c_copy(m, r, g, s).start()

    def crossed(m):
        @pl.when(lane(m))
        def _():
            @pl.loop(0, n_fs)
            def _(o):
                crossed_step(m, o)

    def secondary_step(m, o):
        r = by_way(o)
        for dg in range(1, n_grp):
            h = along_grp(dg)
            for s in range(subs[m]):
                arrived(piece(m, r, h, s), y_recv.at[m, r, h, s])
                c_copy(m, r, h, s).start()

    def secondary(m):
        @pl.when(lane(m))
        def _():
            @pl.loop(0, n_fs)
            def _(o):
                secondary_step(m, o)

    def complete(m, groups):
        @pl.when(other_lane(m))
        def _():
            @pl.loop(0, n_fs)
            def _(o):
                r = by_way(o)
                for dg in groups:
                    for s in range(subs[m]):
                        arrived(piece(m, r, along_grp(dg), s), c_recv.at[m, r, along_grp(dg), s])

    near, far = range(1), range(1, n_grp)
    direct = DIRECT

    def d_piece(k, s, h):
        return served_down[k].at[
            pl.ds(pl.multiple_of(h * d_share, d_share), d_share),
            pl.ds(pl.multiple_of(s * d_cols, d_cols), d_cols),
        ]

    def d_block(k, s):
        return served_down[k].at[:, pl.ds(pl.multiple_of(s * d_cols, d_cols), d_cols)]

    def d_first(k, s):
        return d_block(k, s) if direct[k] else d_piece(k, s, g)

    def dx_copy(k, dx):
        ref = d_first(k, t)
        return remote(ref, ref, dx_send.at[k, dx - 1], dx_recv.at[k, dx - 1], {"tp": along_tp(dx)})

    def dy_copy(k, dx, dg):
        ref = d_piece(k, lax.rem(t + n_tp - 2 * dx, n_tp), g)
        return remote(ref, ref, dy_send.at[k, dx - 1, dg - 1], dy_recv.at[k, dx - 1, dg - 1], {"grp": along_grp(dg)})

    def dc_copy(k, dx):
        ref = d_block(k, lax.rem(t + n_tp - 2 * dx, n_tp))
        return remote(ref, ref, dc_send.at[k, dx], dc_recv.at[k, dx], {"tp": partner})

    def down_start(k):
        for dx in range(1, chips):
            dx_copy(k, dx).start()
        dc_copy(k, 0).start()

    def down_primary(k):
        if direct[k]:
            return
        for dx in range(1, chips):
            source = lax.rem(t + n_tp - 2 * dx, n_tp)
            arrived(d_piece(k, source, g), dx_recv.at[k, dx - 1])
            for dg in range(1, n_grp):
                dy_copy(k, dx, dg).start()

    def down_secondary(k):
        for dx in range(1, chips):
            source = lax.rem(t + n_tp - 2 * dx, n_tp)
            if direct[k]:
                arrived(d_block(k, source), dx_recv.at[k, dx - 1])
            else:
                for dg in range(1, n_grp):
                    arrived(d_piece(k, source, lax.rem(g + n_grp - dg, n_grp)), dy_recv.at[k, dx - 1, dg - 1])
            dc_copy(k, dx).start()
        for dx in range(chips):
            arrived(d_block(k, lax.rem(partner + n_tp - 2 * dx, n_tp)), dc_recv.at[k, dx])

    final = (delta, result)

    def to_middle(k, i):
        return remote(onward.at[k, i], middle.at[k, i], s_send.at[k, i], m_recv.at[k, i], {"fs": toward})

    def to_next(k, i):
        return remote(onward.at[k, i], inward.at[k, i], s_send.at[k, i], u_recv.at[k, i], {"fs": toward})

    def to_outer(k, i):
        ref = final[k].at[i]
        return remote(ref, ref, o_send.at[k, i], o_recv.at[k, i], {"fs": away})

    def place(n):
        i, h = n // halves, lax.rem(n, halves)
        return (
            pl.ds(pl.multiple_of(h * part_rows, part_rows), part_rows),
            pl.ds(pl.multiple_of(i * wide, wide), wide),
        )

    def gather_in(k, i):
        at = pl.ds(pl.multiple_of(i * wide, wide), wide)
        value = jnp.dot(hidden[...], served_down[k][:, at], preferred_element_type=jnp.float32)
        for h in range(halves):
            n = i * halves + h
            own_part = value[h * part_rows : (h + 1) * part_rows]

            @pl.when(is_end)
            def _():
                onward[k, n] = own_part.astype(jnp.bfloat16)

            @pl.when(jnp.logical_not(is_end))
            def _():
                arrived(inward.at[k, n], u_recv.at[k, n])
                onward[k, n] = (own_part + inward[k, n].astype(jnp.float32)).astype(jnp.bfloat16)

            @pl.when(is_mid)
            def _():
                to_middle(k, n).start()

            @pl.when(jnp.logical_not(is_mid))
            def _():
                to_next(k, n).start()

    def spread_out(k, n):
        at = place(n)

        @pl.when(is_mid)
        def _():
            arrived(middle.at[k, n], m_recv.at[k, n])
            total = 0.5 * (onward[k, n].astype(jnp.float32) + middle[k, n].astype(jnp.float32))
            if k == 1:
                total = stream[at] + total
            final[k][n] = total.astype(jnp.bfloat16)

        @pl.when(jnp.logical_not(is_mid))
        def _():
            arrived(final[k].at[n], o_recv.at[k, n])

        @pl.when(jnp.logical_not(is_end))
        def _():
            to_outer(k, n).start()

        if k == 0:
            stream[at] = stream[at] + delta[n].astype(jnp.float32)

    def reduce(k, beside=None):
        lag = jnp.where(is_mid, LAG, chunks)
        first = jnp.where(is_mid, 1, chunks)

        @pl.loop(0, jnp.where(is_mid, chunks + LAG, 2 * chunks))
        def _(i):
            @pl.when(i < chunks)
            def _():
                gather_in(k, i)

            if beside is not None:
                @pl.when(i >= first)
                def _():
                    beside(i - first)

            @pl.when(i >= lag)
            def _():
                for h in range(halves):
                    spread_out(k, (i - lag) * halves + h)

    def norm():
        @pl.loop(0, tokens // slab)
        def _(i):
            at = pl.ds(pl.multiple_of(i * slab, slab), slab)
            value = stream[at]
            factor = lax.rsqrt(jnp.mean(value * value, axis=-1, keepdims=True) + EPS)
            normed[at] = (value * factor).astype(jnp.bfloat16)

    def multiply(k):
        w_gate, w_up = served[2 * k], served[2 * k + 1]

        @pl.loop(0, width // tile)
        def _(i):
            at = pl.ds(pl.multiple_of(i * tile, tile), tile)
            gate = jnp.dot(normed[...], w_gate[:, at], preferred_element_type=jnp.float32)
            up = jnp.dot(normed[...], w_up[:, at], preferred_element_type=jnp.float32)
            hidden[:, at] = (jax.nn.silu(gate) * up).astype(jnp.bfloat16)

    for n in (0, 1, 2, 4):
        load(n).start()
    prompt_copy = pltpu.make_async_copy(prompt, normed, prompt_sem)
    prompt_copy.start()

    barrier = pltpu.get_barrier_semaphore()
    peers = (
        [{"fs": along_fs(o)} for o in range(1, n_fs)]
        + [{"fs": along_fs(o), "tp": partner} for o in range(1, n_fs)]
        + [{"tp": along_tp(dx)} for dx in range(1, chips)]
        + [{"grp": along_grp(dg)} for dg in range(1, n_grp)]
        + [{"tp": partner}]
    )
    for peer in peers:
        pl.semaphore_signal(barrier, inc=1, device_id=peer, device_id_type=MESH)
    spread_gain(0)
    fold(0)
    pl.semaphore_wait(barrier, len(peers))

    p_start(0)
    z_start(0, 0)
    load(3).start()
    fold(1)
    p_start(1)
    z_start(1, 0)
    spread_gain(1)
    fold(2)
    p_start(2)
    round_down(0)
    load(5).start()
    fold(3)
    round_down(1)
    prompt_copy.wait()
    stream[...] = normed[...].astype(jnp.float32)
    norm()

    own_first(0)
    own_first(1)
    relay(0)
    own_later(0)
    primary(0, 1, 2)
    relay(1)
    own_later(1)
    primary(0, 2)
    primary(1)
    z_start(2, 0)
    own_first(2)
    relay(2)
    own_later(2)
    p_start(3)
    z_start(3, 0)
    own_first(3)
    crossed(0)
    crossed(1)
    down_start(0)
    relay(3)
    own_later(3)
    primary(2)
    secondary(0)
    secondary(1)
    for m in (0, 1):
        complete(m, near)
        complete(m, far)
    multiply(0)
    primary(3)
    down_start(1)
    down_secondary(0)

    def beside(i):
        per = -(-n_fs // chunks)
        for q in range(per):
            n = i * per + q

            @pl.when(jnp.logical_and(lane(2), n < n_fs))
            def _():
                secondary_step(2, n)

            @pl.when(jnp.logical_and(lane(3), n < n_fs))
            def _():
                crossed_step(3, n)

    reduce(0, beside)
    norm()
    secondary(3)
    for m in (2, 3):
        complete(m, near)
        complete(m, far)
    multiply(1)
    down_secondary(1)
    reduce(1)

    for m in range(4):
        for s in range(columns_to[m]):
            if s > 0:
                p_copy(m, s).wait_send()
            for j in range(ratio):
                @pl.when(z_copy(m, s, j)[2] != f)
                def _():
                    z_remote(m, s, j).wait_send()

                if m % 2 == 1:
                    @pl.when(z_copy(m, s, j)[2] == f)
                    def _():
                        z_aside(m, s, j).wait_send()

        @pl.when(lane(m))
        def _():
            @pl.loop(0, n_fs)
            def _(r):
                if not WHOLE[m]:
                    @pl.when(carries)
                    def _():
                        for dx in range(1, chips):
                            x_copy(m, r, dx).wait_send()

                for s in range(subs[m]):
                    for dg in range(1, n_grp):
                        y_copy(m, r, dg, s).wait_send()
                    for h in range(n_grp):
                        c_copy(m, r, h, s).wait_send()

    for k in range(2):
        dc_copy(k, 0).wait_send()
        for dx in range(1, chips):
            dx_copy(k, dx).wait_send()
            dc_copy(k, dx).wait_send()
            if not direct[k]:
                for dg in range(1, n_grp):
                    dy_copy(k, dx, dg).wait_send()

        @pl.loop(0, chunks * halves)
        def _(i):
            @pl.when(is_mid)
            def _():
                to_middle(k, i).wait_send()

            @pl.when(jnp.logical_not(is_mid))
            def _():
                to_next(k, i).wait_send()

            @pl.when(jnp.logical_not(is_end))
            def _():
                to_outer(k, i).wait_send()


def store(halves, parts, *refs):
    ins, outs, sems = refs[:7], refs[7:14], refs[14]
    copies = []
    pieces, rows, wide = ins[0].shape
    for n in range(pieces):
        at = pl.ds(n % halves * rows, rows), pl.ds(n // halves * wide, wide)
        copies.append((ins[0].at[n], outs[0].at[at]))
    for src, dst in zip(ins[1:], outs[1:]):
        rows = src.shape[0] // parts
        for i in range(parts):
            at = pl.ds(i * rows, rows)
            copies.append((src.at[at], dst.at[at]))
    copies = [pltpu.make_async_copy(src, dst, sems.at[i]) for i, (src, dst) in enumerate(copies)]
    for copy in copies:
        copy.start()
    for copy in copies:
        copy.wait()


def on_device(
    n_grp, n_fs, n_tp,
    prompt,
    gain_first,
    gate_first,
    up_first,
    down_first,
    gain_second,
    gate_second,
    up_second,
    down_second,
):
    tokens, features = prompt.shape
    rows, columns = gate_first.shape
    width = columns * n_tp // n_fs
    d_rows, d_cols = down_first.shape
    chips = n_tp // 2
    wide = min(256, features)
    halves = HALVES if tokens % (16 * HALVES) == 0 else 1
    chunks = features // wide
    parts = (chunks * halves, tokens // halves, wide)
    gate_shape, down_shape = (features, width), (d_rows, features)
    bf16 = functools.partial(jax.ShapeDtypeStruct, dtype=jnp.bfloat16)
    share = rows // n_grp
    n_sub = chips if share % (16 * chips) == 0 else 1
    other_x, other_g = max(chips - 1, 1), max(n_grp - 1, 1)
    sems = [
        (6,), (),
        (4, other_x), (4, other_x), (4, other_x, n_fs // n_tp),
        (4, n_fs // n_tp), (4, n_fs), (4, n_fs, other_x), (4, n_fs, n_sub), (4, n_fs, other_g, n_sub),
        (4, n_fs, n_grp, n_sub), (4, n_fs, n_grp, n_sub), (4, n_fs, n_grp, n_sub), (4,),
        (2, other_x), (2, other_x), (2, other_x, other_g), (2, other_x, other_g),
        (2, chips), (2, chips),
        *[(2, parts[0])] * 5,
    ]
    if rows % LANES == 0:
        gains = [gain.reshape(1, rows) for gain in (gain_first, gain_second)]
    else:
        gains = [jnp.broadcast_to(gain[:, None], (rows, LANES)) for gain in (gain_first, gain_second)]
    far = functools.partial(pltpu.with_memory_space_constraint, memory_space=pltpu.HBM)
    vmem, hbm = pl.BlockSpec(memory_space=pltpu.VMEM), pl.BlockSpec(memory_space=pltpu.HBM)
    shapes = [parts] + [gate_shape] * 4 + [down_shape] * 2
    held = pl.pallas_call(
        functools.partial(kernel, n_grp, n_fs, n_tp, n_sub),
        out_shape=[bf16(s) for s in shapes],
        in_specs=[hbm] + [vmem] * 2 + [hbm] * 6,
        out_specs=[vmem] * 7,
        scratch_shapes=[
            [pltpu.VMEM((rows, columns), jnp.float32)] * 3 + [pltpu.VMEM((d_rows, d_cols), jnp.float32)],
            pltpu.VMEM((4, rows, columns), jnp.bfloat16),
            pltpu.VMEM((2, rows, LANES), jnp.float32),
            pltpu.VMEM((tokens, features), jnp.float32),
            pltpu.VMEM((tokens, features), jnp.bfloat16),
            pltpu.VMEM((tokens, width), jnp.bfloat16),
            pltpu.VMEM((2, *parts), jnp.bfloat16),
            pltpu.VMEM((2, *parts), jnp.bfloat16),
            pltpu.VMEM((2, *parts), jnp.bfloat16),
            pltpu.VMEM(parts, jnp.bfloat16),
            [
                pltpu.VMEM((other_x, share // (1 if whole else n_sub), columns), jnp.bfloat16)
                for whole in WHOLE
            ],
        ]
        + [pltpu.SemaphoreType.DMA(s) for s in sems],
        compiler_params=pltpu.CompilerParams(
            collective_id=0, has_side_effects=True, vmem_limit_bytes=27 * 2**20
        ),
        name="serve",
    )(far(prompt), *gains, *map(far, (gate_first, up_first, gate_second, up_second, down_first, down_second)))
    result, g1, u1, g2, u2, d1, d2 = pl.pallas_call(
        functools.partial(store, halves, SPLIT),
        out_shape=[bf16((tokens, features))] + [bf16(s) for s in shapes[1:]],
        in_specs=[vmem] * 7,
        out_specs=[hbm] * 7,
        scratch_shapes=[pltpu.SemaphoreType.DMA((parts[0] + 6 * SPLIT,))],
        compiler_params=pltpu.CompilerParams(vmem_limit_bytes=2**20),
        name="store",
    )(*held)
    return (result, g1, u1, d1, g2, u2, d2)
def solution(mesh):
    return jax.shard_map(
        functools.partial(on_device, mesh.shape["grp"], mesh.shape["fs"], mesh.shape["tp"]),
        mesh=mesh,
        in_specs=(
            P(("grp", "tp"), None),
            P("fs"),
            P("fs", "tp"),
            P("fs", "tp"),
            P("fs", "tp"),
            P("fs"),
            P("fs", "tp"),
            P("fs", "tp"),
            P("fs", "tp"),
        ),
        out_specs=(
            P(("grp", "tp"), None),
            P("grp", "fs"),
            P("grp", "fs"),
            P("fs", "grp"),
            P("grp", "fs"),
            P("grp", "fs"),
            P("fs", "grp"),
        ),
        check_vma=False,
    )
```

```python
import functools

import jax
import jax.numpy as jnp
from jax import lax
from jax.experimental import pallas as pl
from jax.experimental.pallas import tpu as pltpu
from jax.sharding import PartitionSpec as P

EPS = 1e-06
MESH = pl.DeviceIdType.MESH
LANES = 128
LAG = 2
LEAD = 3
HALVES = 2
SPLIT = 4
WHOLE = (False, False, False, False)


def kernel(n_grp, n_fs, n_tp, n_sub, *refs):
    prompt, gains, weights, downs = refs[0], refs[1:3], refs[3:7], refs[7:9]
    result, served, served_down = refs[9], refs[10:14], refs[14:16]
    (land, gain_land, own, scale, stream, normed, hidden, onward, inward, middle, delta, stage) = refs[16:28]
    (load_sem, gain_sem, prompt_sem,
     p_send, p_recv, r_send, z_send, z_recv, x_send, x_recv, y_send, y_recv, c_send, c_recv, own_sem,
     dx_send, dx_recv, dc_send, dc_recv,
     s_send, u_recv, m_recv, o_send, o_recv) = refs[28:]

    g, f, t = lax.axis_index("grp"), lax.axis_index("fs"), lax.axis_index("tp")
    ratio = n_fs // n_tp
    chips = n_tp // 2
    home = f // ratio
    mine_sub = lax.rem(t // 2 + chips - home // 2, chips)
    carries = mine_sub < n_sub
    partner = t + 1 - 2 * lax.rem(t, 2)

    def lane(m):
        return lax.rem(t + m, 2) == lax.rem(home, 2)

    def other_lane(m):
        return lax.rem(t + m, 2) != lax.rem(home, 2)

    half = n_fs // 2
    lower = f < half
    is_mid = jnp.logical_or(f == half - 1, f == half)
    is_end = jnp.logical_or(f == 0, f == n_fs - 1)
    toward = jnp.where(lower, f + 1, f - 1)
    away = jnp.where(lower, jnp.maximum(f - 1, 0), jnp.minimum(f + 1, n_fs - 1))

    depth = jnp.where(lower, f, n_fs - 1 - f)

    def along_fs(o):
        return lax.rem(f + o, n_fs)

    def by_way(o):
        r = jnp.where(o <= depth, depth - o, o)
        return jnp.where(lower, r, n_fs - 1 - r)

    def along_tp(dx):
        return lax.rem(t + 2 * dx, n_tp)

    def along_grp(dg):
        return lax.rem(g + dg, n_grp)

    def remote(src, dst, send, recv, where):
        return pltpu.make_async_remote_copy(
            src_ref=src, dst_ref=dst, send_sem=send, recv_sem=recv,
            device_id=where, device_id_type=MESH,
        )

    def arrived(dst, sem):
        pltpu.make_async_copy(dst, dst, sem).wait()

    rows, columns = weights[0].shape
    share = rows // n_grp
    subs = [1 if whole else n_sub for whole in WHOLE]
    columns_to = [chips if whole else n_sub for whole in WHOLE]
    width = served[0].shape[1]
    d_rows, d_cols = downs[0].shape
    tokens, features = prompt.shape
    slab = min(64, tokens)
    tile = min(256, width)
    wide = min(256, features)
    chunks = features // wide
    strips = d_cols // wide
    halves, part_rows, _ = result.shape[0] // chunks, *result.shape[1:]

    def landing(n):
        return land[n % 3] if n < 4 else land[3]

    def load(n):
        src = weights[n] if n < 4 else downs[n - 4]
        return pltpu.make_async_copy(src, landing(n), load_sem.at[n])

    def gain_copy(k):
        return pltpu.make_async_copy(gains[k], gain_land.at[k], gain_sem.at[k])

    def spread_gain(k):
        gain_copy(k).wait()
        gain = gain_land.at[k]
        if gain.shape[0] == rows:
            scale[k] = gain[...]
        else:
            scale[k] = jnp.broadcast_to(gain[...], (LANES, rows)).T

    def fold(m):
        load(m).wait()
        step = min(64, rows)

        @pl.loop(0, rows // step)
        def _(i):
            at = pl.ds(pl.multiple_of(i * step, step), step)
            factor = scale[m // 2, at]
            for j in range(columns // LANES):
                lanes = pl.ds(j * LANES, LANES)
                own[m, at, lanes] = (factor * landing(m)[at, lanes]).astype(jnp.bfloat16)

    def round_down(k):
        load(4 + k).wait()
        step = min(64, d_rows)

        @pl.loop(0, d_rows // step)
        def _(i):
            at = pl.ds(pl.multiple_of(i * step, step), step)
            to = pl.ds(pl.multiple_of(t * d_cols, d_cols), d_cols)
            served_down[k][at, to] = landing(4 + k)[at].astype(jnp.bfloat16)

    def carried(m, s):
        return 0 if WHOLE[m] else s

    def piece(m, r, h, s):
        sub = share // subs[m]
        return served[m].at[pl.ds(pl.multiple_of(r * rows + h * share + s * sub, sub), sub)]

    def own_rows(m, s):
        sub = share // subs[m]
        return pl.ds(pl.multiple_of(g * share + carried(m, s) * sub, sub), sub)

    def p_copy(m, s):
        src = own.at[m, own_rows(m, s)]
        return remote(src, stage[m].at[s - 1], p_send.at[m, s - 1], p_recv.at[m, s - 1], {"tp": along_tp(s)})

    def p_start(m):
        for s in range(1, columns_to[m]):
            p_copy(m, s).start()

    def z_copy(m, s, j):
        cut = pl.ds(j * width, width)
        if s == 0:
            return own.at[m, own_rows(m, 0), cut], piece(m, f, g, 0), t * ratio + j
        source = lax.rem(t + n_tp - 2 * s, n_tp)
        return stage[m].at[s - 1, :, cut], piece(m, f, g, carried(m, s)), source * ratio + j

    def z_remote(m, s, j):
        src, dst, to = z_copy(m, s, j)
        send = z_send.at[m, j] if s == 0 else r_send.at[m, s - 1, j]
        where = {"fs": to} if m % 2 == 0 else {"fs": to, "tp": partner}
        return remote(src, dst, send, z_recv.at[m, f], where)

    def z_aside(m, s, j):
        src, dst, _ = z_copy(m, s, j)
        send = z_send.at[m, j] if s == 0 else r_send.at[m, s - 1, j]
        return remote(src, dst, send, own_sem.at[m], {"tp": partner})

    def z_start(m, s):
        for j in range(ratio):
            src, dst, to = z_copy(m, s, j)

            @pl.when(to != f)
            def _():
                z_remote(m, s, j).start()

            @pl.when(to == f)
            def _():
                if m % 2 == 0:
                    pltpu.make_async_copy(src, dst, own_sem.at[m]).start()
                else:
                    z_aside(m, s, j).start()

    def relay(m):
        for s in range(1, columns_to[m]):
            arrived(stage[m].at[s - 1], p_recv.at[m, s - 1])
            z_start(m, s)

    def x_copy(m, r, dx):
        ref = piece(m, r, g, mine_sub)
        return remote(ref, ref, x_send.at[m, r, dx - 1], x_recv.at[m, r, mine_sub], {"tp": along_tp(dx)})

    def y_copy(m, r, dg, s):
        ref = piece(m, r, g, s)
        return remote(ref, ref, y_send.at[m, r, dg - 1, s], y_recv.at[m, r, g, s], {"grp": along_grp(dg)})

    def c_copy(m, r, h, s):
        ref = piece(m, r, h, s)
        return remote(ref, ref, c_send.at[m, r, h, s], c_recv.at[m, r, h, s], {"tp": partner})

    def primary_step(m, o):
        r = by_way(o)
        s = 0 if WHOLE[m] else mine_sub
        ref = piece(m, r, g, s)

        def onward_from(first):
            arrived(ref, own_sem.at[m] if first else z_recv.at[m, r])
            if not WHOLE[m]:
                for dx in range(1, chips):
                    x_copy(m, r, dx).start()
            for dg in range(1, n_grp):
                y_copy(m, r, dg, s).start()
            c_copy(m, r, g, s).start()

        if WHOLE[m]:
            onward_from(isinstance(o, int))
        else:
            @pl.when(carries)
            def _():
                onward_from(isinstance(o, int))

    def own_first(m):
        @pl.when(jnp.logical_and(lane(m), mine_sub == 0))
        def _():
            primary_step(m, 0)

    def own_later(m):
        @pl.when(jnp.logical_and(lane(m), mine_sub != 0))
        def _():
            primary_step(m, 0)

    straight = mine_sub == 0

    def primary(m, where=True, low=1, high=n_fs):
        @pl.when(jnp.logical_and(lane(m), where))
        def _():
            @pl.loop(low, high)
            def _(o):
                primary_step(m, o)

    def crossed_step(m, o):
        r = by_way(o)
        for s in range(0 if WHOLE[m] else n_sub):
            @pl.when(mine_sub != s)
            def _():
                arrived(piece(m, r, g, s), x_recv.at[m, r, s])
                for dg in range(1, n_grp):
                    y_copy(m, r, dg, s).start()
                c_copy(m, r, g, s).start()

    def crossed(m, low=0, high=n_fs):
        @pl.when(lane(m))
        def _():
            @pl.loop(low, high)
            def _(o):
                crossed_step(m, o)

    def secondary_step(m, o):
        r = by_way(o)
        for dg in range(1, n_grp):
            h = along_grp(dg)
            for s in range(subs[m]):
                arrived(piece(m, r, h, s), y_recv.at[m, r, h, s])
                c_copy(m, r, h, s).start()

    def secondary(m):
        @pl.when(lane(m))
        def _():
            @pl.loop(0, n_fs)
            def _(o):
                secondary_step(m, o)

    def complete(m, groups):
        @pl.when(other_lane(m))
        def _():
            @pl.loop(0, n_fs)
            def _(o):
                r = by_way(o)
                for dg in groups:
                    for s in range(subs[m]):
                        arrived(piece(m, r, along_grp(dg), s), c_recv.at[m, r, along_grp(dg), s])

    near, far = range(1), range(1, n_grp)

    def d_strip(k, s, j):
        return served_down[k].at[:, pl.ds(pl.multiple_of(s * d_cols + j * wide, wide), wide)]

    def d_from(device, dx):
        return lax.rem(device + n_tp - 2 * dx, n_tp)

    def dx_copy(k, dx, j):
        ref = d_strip(k, t, j)
        return remote(ref, ref, dx_send.at[k, dx - 1, j], dx_recv.at[k, dx - 1, j], {"tp": along_tp(dx)})

    def dc_copy(k, dx, j):
        ref = d_strip(k, d_from(t, dx), j)
        return remote(ref, ref, dc_send.at[k, dx, j], dc_recv.at[k, dx, j], {"tp": partner})

    def down_start(k):
        for j in range(strips):
            for dx in range(1, chips):
                dx_copy(k, dx, j).start()
            dc_copy(k, 0, j).start()

    def down_pass(k, dx, j):
        arrived(d_strip(k, d_from(t, dx), j), dx_recv.at[k, dx - 1, j])
        dc_copy(k, dx, j).start()

    def down_ready(k, dx, j):
        arrived(d_strip(k, d_from(partner, dx), j), dc_recv.at[k, dx, j])

    final = (delta, result)

    def to_middle(k, i):
        return remote(onward.at[k, i], middle.at[k, i], s_send.at[k, i], m_recv.at[k, i], {"fs": toward})

    def to_next(k, i):
        return remote(onward.at[k, i], inward.at[k, i], s_send.at[k, i], u_recv.at[k, i], {"fs": toward})

    def to_outer(k, i):
        ref = final[k].at[i]
        return remote(ref, ref, o_send.at[k, i], o_recv.at[k, i], {"fs": away})

    def place(n):
        i, h = n // halves, lax.rem(n, halves)
        return (
            pl.ds(pl.multiple_of(h * part_rows, part_rows), part_rows),
            pl.ds(pl.multiple_of(i * wide, wide), wide),
        )

    def gather_in(k, i):
        at = pl.ds(pl.multiple_of(i * wide, wide), wide)
        value = jnp.dot(hidden[...], served_down[k][:, at], preferred_element_type=jnp.float32)
        for h in range(halves):
            n = i * halves + h
            own_part = value[h * part_rows : (h + 1) * part_rows]

            @pl.when(is_end)
            def _():
                onward[k, n] = own_part.astype(jnp.bfloat16)

            @pl.when(jnp.logical_not(is_end))
            def _():
                arrived(inward.at[k, n], u_recv.at[k, n])
                onward[k, n] = (own_part + inward[k, n].astype(jnp.float32)).astype(jnp.bfloat16)

            @pl.when(is_mid)
            def _():
                to_middle(k, n).start()

            @pl.when(jnp.logical_not(is_mid))
            def _():
                to_next(k, n).start()

    def spread_out(k, n):
        at = place(n)

        @pl.when(is_mid)
        def _():
            arrived(middle.at[k, n], m_recv.at[k, n])
            total = 0.5 * (onward[k, n].astype(jnp.float32) + middle[k, n].astype(jnp.float32))
            if k == 1:
                total = stream[at] + total
            final[k][n] = total.astype(jnp.bfloat16)

        @pl.when(jnp.logical_not(is_mid))
        def _():
            arrived(final[k].at[n], o_recv.at[k, n])

        @pl.when(jnp.logical_not(is_end))
        def _():
            to_outer(k, n).start()

        if k == 0:
            stream[at] = stream[at] + delta[n].astype(jnp.float32)

    per_chip = chunks // chips

    def chunk_of(i):
        chip = lax.rem(t // 2 + chips - i // per_chip, chips)
        j = lax.rem(i, per_chip)
        return chip * per_chip + lax.rem(j, 2) * strips + j // 2

    def reduce(k, beside=None):
        lag = jnp.where(is_mid, LAG, chunks)
        first = jnp.where(is_end, LEAD, 1)

        @pl.loop(0, jnp.where(is_mid, chunks + LAG, 2 * chunks))
        def _(i):
            if beside is not None:
                @pl.when(i >= first)
                def _():
                    beside(i - first)

            @pl.when(i < chunks)
            def _():
                for dx in range(1, chips):
                    for j in range(strips):
                        @pl.when(i == dx * per_chip + 2 * j - 1)
                        def _():
                            down_pass(k, dx, j)

                        @pl.when(i == dx * per_chip + 2 * j)
                        def _():
                            down_ready(k, dx, j)

                gather_in(k, chunk_of(i))

            @pl.when(i >= lag)
            def _():
                for h in range(halves):
                    spread_out(k, chunk_of(i - lag) * halves + h)

    def norm():
        @pl.loop(0, tokens // slab)
        def _(i):
            at = pl.ds(pl.multiple_of(i * slab, slab), slab)
            value = stream[at]
            factor = lax.rsqrt(jnp.mean(value * value, axis=-1, keepdims=True) + EPS)
            normed[at] = (value * factor).astype(jnp.bfloat16)

    def multiply(k):
        w_gate, w_up = served[2 * k], served[2 * k + 1]

        @pl.loop(0, width // tile)
        def _(i):
            at = pl.ds(pl.multiple_of(i * tile, tile), tile)
            gate = jnp.dot(normed[...], w_gate[:, at], preferred_element_type=jnp.float32)
            up = jnp.dot(normed[...], w_up[:, at], preferred_element_type=jnp.float32)
            hidden[:, at] = (jax.nn.silu(gate) * up).astype(jnp.bfloat16)

    gain_copy(0).start()
    for n in (0, 1, 2, 4):
        load(n).start()
    gain_copy(1).start()
    prompt_copy = pltpu.make_async_copy(prompt, normed, prompt_sem)
    prompt_copy.start()

    barrier = pltpu.get_barrier_semaphore()
    peers = (
        [{"fs": along_fs(o)} for o in range(1, n_fs)]
        + [{"fs": along_fs(o), "tp": partner} for o in range(1, n_fs)]
        + [{"tp": along_tp(dx)} for dx in range(1, chips)]
        + [{"grp": along_grp(dg)} for dg in range(1, n_grp)]
        + [{"tp": partner}]
    )
    for peer in peers:
        pl.semaphore_signal(barrier, inc=1, device_id=peer, device_id_type=MESH)
    spread_gain(0)
    fold(0)
    pl.semaphore_wait(barrier, len(peers))

    p_start(0)
    z_start(0, 0)
    load(3).start()
    fold(1)
    p_start(1)
    z_start(1, 0)
    spread_gain(1)
    fold(2)
    round_down(0)
    load(5).start()
    fold(3)
    round_down(1)
    prompt_copy.wait()
    stream[...] = normed[...].astype(jnp.float32)
    norm()

    own_first(0)
    own_first(1)
    relay(0)
    own_later(0)
    relay(1)
    own_later(1)
    primary(0, True, 1, 2)
    primary(1, True, 1, 2)
    crossed(0, 0, 1)
    crossed(1, 0, 1)
    primary(0, True, 2)
    primary(1, True, 2)
    p_start(2)
    z_start(2, 0)
    crossed(0, 1)
    crossed(1, 1)
    p_start(3)
    z_start(3, 0)
    down_start(0)
    complete(0, near)
    complete(1, near)
    relay(2)
    own_first(2)
    secondary(0)
    relay(3)
    own_later(2)
    primary(2, straight)
    secondary(1)
    complete(0, far)
    complete(1, far)
    multiply(0)
    own_first(3)
    own_later(3)
    primary(3, straight)
    for j in range(strips):
        down_ready(0, 0, j)

    crooked = jnp.logical_not(straight)

    def beside(i):
        @pl.when(i == 0)
        def _():
            primary(2, crooked)
            primary(3, crooked)

        @pl.when(i == 3)
        def _():
            down_start(1)

        per = -(-n_fs // 4)
        for m in (2, 3):
            for q in range(per):
                n = i // 2 * per + q

                @pl.when(jnp.logical_and(lane(m), jnp.logical_and(lax.rem(i, 2) == 1, n < n_fs)))
                def _():
                    crossed_step(m, n)

    reduce(0, beside)
    norm()
    secondary(2)
    secondary(3)
    for m in (2, 3):
        complete(m, near)
        complete(m, far)
    multiply(1)
    for j in range(strips):
        down_ready(1, 0, j)
    reduce(1)

    for m in range(4):
        for s in range(columns_to[m]):
            if s > 0:
                p_copy(m, s).wait_send()
            for j in range(ratio):
                @pl.when(z_copy(m, s, j)[2] != f)
                def _():
                    z_remote(m, s, j).wait_send()

                if m % 2 == 1:
                    @pl.when(z_copy(m, s, j)[2] == f)
                    def _():
                        z_aside(m, s, j).wait_send()

        @pl.when(lane(m))
        def _():
            @pl.loop(0, n_fs)
            def _(r):
                if not WHOLE[m]:
                    @pl.when(carries)
                    def _():
                        for dx in range(1, chips):
                            x_copy(m, r, dx).wait_send()

                for s in range(subs[m]):
                    for dg in range(1, n_grp):
                        y_copy(m, r, dg, s).wait_send()
                    for h in range(n_grp):
                        c_copy(m, r, h, s).wait_send()

    for k in range(2):
        for j in range(strips):
            dc_copy(k, 0, j).wait_send()
            for dx in range(1, chips):
                dx_copy(k, dx, j).wait_send()
                dc_copy(k, dx, j).wait_send()

        @pl.loop(0, chunks * halves)
        def _(i):
            @pl.when(is_mid)
            def _():
                to_middle(k, i).wait_send()

            @pl.when(jnp.logical_not(is_mid))
            def _():
                to_next(k, i).wait_send()

            @pl.when(jnp.logical_not(is_end))
            def _():
                to_outer(k, i).wait_send()


def store(halves, parts, *refs):
    ins, outs, sems = refs[:7], refs[7:14], refs[14]
    copies = []
    pieces, rows, wide = ins[0].shape
    for n in range(pieces):
        at = pl.ds(n % halves * rows, rows), pl.ds(n // halves * wide, wide)
        copies.append((ins[0].at[n], outs[0].at[at]))
    for src, dst in zip(ins[1:], outs[1:]):
        rows = src.shape[0] // parts
        for i in range(parts):
            at = pl.ds(i * rows, rows)
            copies.append((src.at[at], dst.at[at]))
    copies = [pltpu.make_async_copy(src, dst, sems.at[i]) for i, (src, dst) in enumerate(copies)]
    for copy in copies:
        copy.start()
    for copy in copies:
        copy.wait()


def on_device(
    n_grp, n_fs, n_tp,
    prompt,
    gain_first,
    gate_first,
    up_first,
    down_first,
    gain_second,
    gate_second,
    up_second,
    down_second,
):
    tokens, features = prompt.shape
    rows, columns = gate_first.shape
    width = columns * n_tp // n_fs
    d_rows, d_cols = down_first.shape
    chips = n_tp // 2
    wide = min(256, features)
    halves = HALVES if tokens % (16 * HALVES) == 0 else 1
    chunks = features // wide
    parts = (chunks * halves, tokens // halves, wide)
    strips = d_cols // wide
    gate_shape, down_shape = (features, width), (d_rows, features)
    bf16 = functools.partial(jax.ShapeDtypeStruct, dtype=jnp.bfloat16)
    share = rows // n_grp
    n_sub = chips if share % (16 * chips) == 0 else 1
    other_x, other_g = max(chips - 1, 1), max(n_grp - 1, 1)
    sems = [
        (6,), (2,), (),
        (4, other_x), (4, other_x), (4, other_x, n_fs // n_tp),
        (4, n_fs // n_tp), (4, n_fs), (4, n_fs, other_x), (4, n_fs, n_sub), (4, n_fs, other_g, n_sub),
        (4, n_fs, n_grp, n_sub), (4, n_fs, n_grp, n_sub), (4, n_fs, n_grp, n_sub), (4,),
        (2, other_x, strips), (2, other_x, strips), (2, chips, strips), (2, chips, strips),
        *[(2, parts[0])] * 5,
    ]
    if rows % LANES == 0:
        gains = [gain.reshape(1, rows) for gain in (gain_first, gain_second)]
    else:
        gains = [jnp.broadcast_to(gain[:, None], (rows, LANES)) for gain in (gain_first, gain_second)]
    far = functools.partial(pltpu.with_memory_space_constraint, memory_space=pltpu.HBM)
    vmem, hbm = pl.BlockSpec(memory_space=pltpu.VMEM), pl.BlockSpec(memory_space=pltpu.HBM)
    shapes = [parts] + [gate_shape] * 4 + [down_shape] * 2
    held = pl.pallas_call(
        functools.partial(kernel, n_grp, n_fs, n_tp, n_sub),
        out_shape=[bf16(s) for s in shapes],
        in_specs=[hbm] * 9,
        out_specs=[vmem] * 7,
        scratch_shapes=[
            [pltpu.VMEM((rows, columns), jnp.float32)] * 3 + [pltpu.VMEM((d_rows, d_cols), jnp.float32)],
            pltpu.VMEM((2, *gains[0].shape), jnp.float32),
            pltpu.VMEM((4, rows, columns), jnp.bfloat16),
            pltpu.VMEM((2, rows, LANES), jnp.float32),
            pltpu.VMEM((tokens, features), jnp.float32),
            pltpu.VMEM((tokens, features), jnp.bfloat16),
            pltpu.VMEM((tokens, width), jnp.bfloat16),
            pltpu.VMEM((2, *parts), jnp.bfloat16),
            pltpu.VMEM((2, *parts), jnp.bfloat16),
            pltpu.VMEM((2, *parts), jnp.bfloat16),
            pltpu.VMEM(parts, jnp.bfloat16),
            [
                pltpu.VMEM((other_x, share // (1 if whole else n_sub), columns), jnp.bfloat16)
                for whole in WHOLE
            ],
        ]
        + [pltpu.SemaphoreType.DMA(s) for s in sems],
        compiler_params=pltpu.CompilerParams(
            collective_id=0, has_side_effects=True, vmem_limit_bytes=27 * 2**20
        ),
        name="serve",
    )(far(prompt), *map(far, gains), *map(far, (gate_first, up_first, gate_second, up_second, down_first, down_second)))
    result, g1, u1, g2, u2, d1, d2 = pl.pallas_call(
        functools.partial(store, halves, SPLIT),
        out_shape=[bf16((tokens, features))] + [bf16(s) for s in shapes[1:]],
        in_specs=[vmem] * 7,
        out_specs=[hbm] * 7,
        scratch_shapes=[pltpu.SemaphoreType.DMA((parts[0] + 6 * SPLIT,))],
        compiler_params=pltpu.CompilerParams(vmem_limit_bytes=2**20),
        name="store",
    )(*held)
    return (result, g1, u1, d1, g2, u2, d2)
def solution(mesh):
    return jax.shard_map(
        functools.partial(on_device, mesh.shape["grp"], mesh.shape["fs"], mesh.shape["tp"]),
        mesh=mesh,
        in_specs=(
            P(("grp", "tp"), None),
            P("fs"),
            P("fs", "tp"),
            P("fs", "tp"),
            P("fs", "tp"),
            P("fs"),
            P("fs", "tp"),
            P("fs", "tp"),
            P("fs", "tp"),
        ),
        out_specs=(
            P(("grp", "tp"), None),
            P("grp", "fs"),
            P("grp", "fs"),
            P("fs", "grp"),
            P("grp", "fs"),
            P("grp", "fs"),
            P("fs", "grp"),
        ),
        check_vma=False,
    )
```

```python
import functools

import jax
import jax.numpy as jnp
from jax import lax
from jax.experimental import pallas as pl
from jax.experimental.pallas import tpu as pltpu
from jax.sharding import PartitionSpec as P

EPS = 1e-06
MESH = pl.DeviceIdType.MESH
LANES = 128
LAG = 1
LEAD = 3
HALVES = 2
SPLIT = 4
WHOLE = (False, False, False, False)


def kernel(n_grp, n_fs, n_tp, n_sub, *refs):
    prompt, gains, weights, downs = refs[0], refs[1:3], refs[3:7], refs[7:9]
    result, served, served_down = refs[9], refs[10:14], refs[14:16]
    (land, gain_land, own, scale, stream, normed, hidden, opened, onward, inward, middle, delta, stage) = refs[16:29]
    (load_sem, gain_sem, prompt_sem,
     p_send, p_recv, r_send, z_send, z_recv, x_send, x_recv, y_send, y_recv, c_send, c_recv, own_sem,
     dx_send, dx_recv, dc_send, dc_recv,
     s_send, u_recv, back, o_send) = refs[29:]

    g, f, t = lax.axis_index("grp"), lax.axis_index("fs"), lax.axis_index("tp")
    ratio = n_fs // n_tp
    chips = n_tp // 2
    home = f // ratio
    mine_sub = lax.rem(t // 2 + chips - home // 2, chips)
    carries = mine_sub < n_sub
    partner = t + 1 - 2 * lax.rem(t, 2)

    def lane(m):
        return lax.rem(t + m, 2) == lax.rem(home, 2)

    def other_lane(m):
        return lax.rem(t + m, 2) != lax.rem(home, 2)

    half = n_fs // 2
    lower = f < half
    is_mid = jnp.logical_or(f == half - 1, f == half)
    is_end = jnp.logical_or(f == 0, f == n_fs - 1)
    toward = jnp.where(lower, f + 1, f - 1)
    away = jnp.where(lower, jnp.maximum(f - 1, 0), jnp.minimum(f + 1, n_fs - 1))

    depth = jnp.where(lower, f, n_fs - 1 - f)

    def along_fs(o):
        return lax.rem(f + o, n_fs)

    def by_way(o):
        r = jnp.where(o <= depth, depth - o, o)
        return jnp.where(lower, r, n_fs - 1 - r)

    def along_tp(dx):
        return lax.rem(t + 2 * dx, n_tp)

    def along_grp(dg):
        return lax.rem(g + dg, n_grp)

    def remote(src, dst, send, recv, where):
        return pltpu.make_async_remote_copy(
            src_ref=src, dst_ref=dst, send_sem=send, recv_sem=recv,
            device_id=where, device_id_type=MESH,
        )

    def arrived(dst, sem):
        pltpu.make_async_copy(dst, dst, sem).wait()

    rows, columns = weights[0].shape
    share = rows // n_grp
    subs = [1 if whole else n_sub for whole in WHOLE]
    columns_to = [chips if whole else n_sub for whole in WHOLE]
    width = served[0].shape[1]
    d_rows, d_cols = downs[0].shape
    tokens, features = prompt.shape
    slab = min(64, tokens)
    tile = min(256, width)
    wide = min(256, features)
    chunks = features // wide
    strips = d_cols // wide
    halves, part_rows, _ = result.shape[0] // chunks, *result.shape[1:]

    def landing(n):
        return land[n % 3] if n < 4 else land[3]

    def load(n):
        src = weights[n] if n < 4 else downs[n - 4]
        return pltpu.make_async_copy(src, landing(n), load_sem.at[n])

    def gain_copy(k):
        return pltpu.make_async_copy(gains[k], gain_land.at[k], gain_sem.at[k])

    def spread_gain(k):
        gain_copy(k).wait()
        gain = gain_land.at[k]
        if gain.shape[0] == rows:
            scale[k] = gain[...]
        else:
            scale[k] = jnp.broadcast_to(gain[...], (LANES, rows)).T

    def fold(m):
        load(m).wait()
        step = min(64, rows)

        @pl.loop(0, rows // step)
        def _(i):
            at = pl.ds(pl.multiple_of(i * step, step), step)
            factor = scale[m // 2, at]
            for j in range(columns // LANES):
                lanes = pl.ds(j * LANES, LANES)
                own[m, at, lanes] = (factor * landing(m)[at, lanes]).astype(jnp.bfloat16)

    def round_down(k):
        load(4 + k).wait()
        step = min(64, d_rows)

        @pl.loop(0, d_rows // step)
        def _(i):
            at = pl.ds(pl.multiple_of(i * step, step), step)
            to = pl.ds(pl.multiple_of(t * d_cols, d_cols), d_cols)
            served_down[k][at, to] = landing(4 + k)[at].astype(jnp.bfloat16)

    def carried(m, s):
        return 0 if WHOLE[m] else s

    def piece(m, r, h, s):
        sub = share // subs[m]
        return served[m].at[pl.ds(pl.multiple_of(r * rows + h * share + s * sub, sub), sub)]

    def rows_of(m, count):
        return served[m].at[pl.ds(0, count)]

    def own_rows(m, s):
        sub = share // subs[m]
        return pl.ds(pl.multiple_of(g * share + carried(m, s) * sub, sub), sub)

    def p_copy(m, s):
        src = own.at[m, own_rows(m, s)]
        return remote(src, stage[m].at[s - 1], p_send.at[m, s - 1], p_recv.at[m, s - 1], {"tp": along_tp(s)})

    def p_start(m):
        for s in range(1, columns_to[m]):
            p_copy(m, s).start()

    def z_copy(m, s, j):
        cut = pl.ds(j * width, width)
        if s == 0:
            return own.at[m, own_rows(m, 0), cut], piece(m, f, g, 0), t * ratio + j
        source = lax.rem(t + n_tp - 2 * s, n_tp)
        return stage[m].at[s - 1, :, cut], piece(m, f, g, carried(m, s)), source * ratio + j

    def z_remote(m, s, j):
        src, dst, to = z_copy(m, s, j)
        send = z_send.at[m, j] if s == 0 else r_send.at[m, s - 1, j]
        where = {"fs": to} if m % 2 == 0 else {"fs": to, "tp": partner}
        return remote(src, dst, send, z_recv.at[m, f], where)

    def z_aside(m, s, j):
        src, dst, _ = z_copy(m, s, j)
        send = z_send.at[m, j] if s == 0 else r_send.at[m, s - 1, j]
        return remote(src, dst, send, own_sem.at[m], {"tp": partner})

    def z_start(m, s):
        for j in range(ratio):
            src, dst, to = z_copy(m, s, j)

            @pl.when(to != f)
            def _():
                z_remote(m, s, j).start()

            @pl.when(to == f)
            def _():
                if m % 2 == 0:
                    pltpu.make_async_copy(src, dst, own_sem.at[m]).start()
                else:
                    z_aside(m, s, j).start()

    def relay(m):
        for s in range(1, columns_to[m]):
            arrived(stage[m].at[s - 1], p_recv.at[m, s - 1])
            z_start(m, s)

    def x_copy(m, r, dx):
        ref = piece(m, r, g, mine_sub)
        return remote(ref, ref, x_send.at[m], x_recv.at[m, r, mine_sub], {"tp": along_tp(dx)})

    def y_copy(m, r, dg, s):
        ref = piece(m, r, g, s)
        return remote(ref, ref, y_send.at[m], y_recv.at[m, r, dg - 1, s], {"grp": along_grp(dg)})

    def c_copy(m, r, h, s):
        ref = piece(m, r, h, s)
        return remote(ref, ref, c_send.at[m], c_recv.at[m, h], {"tp": partner})

    def primary_step(m, o):
        r = by_way(o)
        s = 0 if WHOLE[m] else mine_sub
        ref = piece(m, r, g, s)

        def onward_from(first):
            arrived(ref, own_sem.at[m] if first else z_recv.at[m, r])
            if not WHOLE[m]:
                for dx in range(1, chips):
                    x_copy(m, r, dx).start()
            for dg in range(1, n_grp):
                y_copy(m, r, dg, s).start()
            c_copy(m, r, g, s).start()

        if WHOLE[m]:
            onward_from(isinstance(o, int))
        else:
            @pl.when(carries)
            def _():
                onward_from(isinstance(o, int))

    def own_first(m):
        @pl.when(jnp.logical_and(lane(m), mine_sub == 0))
        def _():
            primary_step(m, 0)

    def own_later(m):
        @pl.when(jnp.logical_and(lane(m), mine_sub != 0))
        def _():
            primary_step(m, 0)

    straight = mine_sub == 0
    crooked = mine_sub != 0

    def primary(m, where=True, low=1, high=n_fs):
        @pl.when(jnp.logical_and(lane(m), where))
        def _():
            @pl.loop(low, high)
            def _(o):
                primary_step(m, o)

    def crossed_step(m, o):
        r = by_way(o)
        for s in range(0 if WHOLE[m] else n_sub):
            @pl.when(mine_sub != s)
            def _():
                arrived(piece(m, r, g, s), x_recv.at[m, r, s])
                for dg in range(1, n_grp):
                    y_copy(m, r, dg, s).start()
                c_copy(m, r, g, s).start()

    def crossed(m, low=0, high=n_fs):
        @pl.when(lane(m))
        def _():
            @pl.loop(low, high)
            def _(o):
                crossed_step(m, o)

    def secondary_step(m, o):
        r = by_way(o)
        for dg in range(1, n_grp):
            h = along_grp(dg)
            for s in range(subs[m]):
                arrived(piece(m, r, h, s), y_recv.at[m, r, n_grp - dg - 1, s])
                c_copy(m, r, h, s).start()

    def secondary(m, where=True):
        @pl.when(jnp.logical_and(lane(m), where))
        def _():
            @pl.loop(0, n_fs)
            def _(o):
                secondary_step(m, o)

    def complete(m, groups):
        @pl.when(other_lane(m))
        def _():
            for dg in groups:
                arrived(rows_of(m, n_fs * share), c_recv.at[m, along_grp(dg)])

    near, far = range(1), range(1, n_grp)

    def d_strip(k, s, j):
        return served_down[k].at[:, pl.ds(pl.multiple_of(s * d_cols + j * wide, wide), wide)]

    def d_from(device, dx):
        return lax.rem(device + n_tp - 2 * dx, n_tp)

    def dx_copy(k, dx, j):
        ref = d_strip(k, t, j)
        return remote(ref, ref, dx_send.at[k, dx - 1, j], dx_recv.at[k, dx - 1, j], {"tp": along_tp(dx)})

    def dc_copy(k, dx, j):
        ref = d_strip(k, d_from(t, dx), j)
        return remote(ref, ref, dc_send.at[k, dx, j], dc_recv.at[k, dx, j], {"tp": partner})

    def down_start(k):
        for j in range(strips):
            for dx in range(1, chips):
                dx_copy(k, dx, j).start()
            dc_copy(k, 0, j).start()

    def down_pass(k, dx, j):
        arrived(d_strip(k, d_from(t, dx), j), dx_recv.at[k, dx - 1, j])
        dc_copy(k, dx, j).start()

    def down_ready(k, dx, j):
        arrived(d_strip(k, d_from(partner, dx), j), dc_recv.at[k, dx, j])

    final = (delta, result)

    def to_middle(k, i):
        return remote(onward.at[k, i], middle.at[k, i], s_send.at[k], back.at[k, i], {"fs": toward})

    def to_next(k, i):
        return remote(onward.at[k, i], inward.at[k, i], s_send.at[k], u_recv.at[k, i], {"fs": toward})

    def to_outer(k, i):
        ref = final[k].at[i]
        return remote(ref, ref, o_send.at[k], back.at[k, i], {"fs": away})

    def place(n):
        i, h = n // halves, lax.rem(n, halves)
        return (
            pl.ds(pl.multiple_of(h * part_rows, part_rows), part_rows),
            pl.ds(pl.multiple_of(i * wide, wide), wide),
        )

    def gather_in(k, i):
        at = pl.ds(pl.multiple_of(i * wide, wide), wide)
        value = jnp.dot(hidden[...], served_down[k][:, at], preferred_element_type=jnp.float32)
        for h in range(halves):
            n = i * halves + h
            own_part = value[h * part_rows : (h + 1) * part_rows]

            @pl.when(is_end)
            def _():
                onward[k, n] = own_part.astype(jnp.bfloat16)

            @pl.when(jnp.logical_not(is_end))
            def _():
                arrived(inward.at[k, n], u_recv.at[k, n])
                onward[k, n] = (own_part + inward[k, n].astype(jnp.float32)).astype(jnp.bfloat16)

            @pl.when(is_mid)
            def _():
                to_middle(k, n).start()

            @pl.when(jnp.logical_not(is_mid))
            def _():
                to_next(k, n).start()

    def spread_out(k, n):
        at = place(n)

        @pl.when(is_mid)
        def _():
            arrived(middle.at[k, n], back.at[k, n])
            total = 0.5 * (onward[k, n].astype(jnp.float32) + middle[k, n].astype(jnp.float32))
            if k == 1:
                total = stream[at] + total
            final[k][n] = total.astype(jnp.bfloat16)

        @pl.when(jnp.logical_not(is_mid))
        def _():
            arrived(final[k].at[n], back.at[k, n])

        @pl.when(jnp.logical_not(is_end))
        def _():
            to_outer(k, n).start()

        if k == 0:
            stream[at] = stream[at] + delta[n].astype(jnp.float32)

    per_chip = chunks // chips

    def chunk_of(i):
        chip = lax.rem(t // 2 + chips - i // per_chip, chips)
        j = lax.rem(i, per_chip)
        return chip * per_chip + lax.rem(j, 2) * strips + j // 2

    def reduce(k, beside=None):
        lag = jnp.where(is_mid, LAG, chunks)
        first = jnp.where(is_end, LEAD, 1)

        @pl.loop(0, jnp.where(is_mid, chunks + LAG, 2 * chunks))
        def _(i):
            if beside is not None:
                @pl.when(i >= first)
                def _():
                    beside(i - first)

            @pl.when(i < chunks)
            def _():
                for dx in range(1, chips):
                    for j in range(strips):
                        @pl.when(i == dx * per_chip + 2 * j - 1)
                        def _():
                            down_pass(k, dx, j)

                        @pl.when(i == dx * per_chip + 2 * j)
                        def _():
                            down_ready(k, dx, j)

                gather_in(k, chunk_of(i))

            @pl.when(i >= lag)
            def _():
                for h in range(halves):
                    spread_out(k, chunk_of(i - lag) * halves + h)

    def norm():
        @pl.loop(0, tokens // slab)
        def _(i):
            at = pl.ds(pl.multiple_of(i * slab, slab), slab)
            value = stream[at]
            factor = lax.rsqrt(jnp.mean(value * value, axis=-1, keepdims=True) + EPS)
            normed[at] = (value * factor).astype(jnp.bfloat16)

    def gate_part(k):
        @pl.loop(0, width // tile)
        def _(i):
            at = pl.ds(pl.multiple_of(i * tile, tile), tile)
            gate = jnp.dot(normed[...], served[2 * k][:, at], preferred_element_type=jnp.float32)
            opened[:, at] = jax.nn.silu(gate)

    def up_part(k):
        @pl.loop(0, width // tile)
        def _(i):
            at = pl.ds(pl.multiple_of(i * tile, tile), tile)
            up = jnp.dot(normed[...], served[2 * k + 1][:, at], preferred_element_type=jnp.float32)
            hidden[:, at] = (opened[:, at] * up).astype(jnp.bfloat16)

    gain_copy(0).start()
    for n in (0, 1, 2, 4):
        load(n).start()
    gain_copy(1).start()
    prompt_copy = pltpu.make_async_copy(prompt, normed, prompt_sem)
    prompt_copy.start()

    barrier = pltpu.get_barrier_semaphore()
    peers = (
        [{"fs": along_fs(o)} for o in range(1, n_fs)]
        + [{"fs": along_fs(o), "tp": partner} for o in range(1, n_fs)]
        + [{"tp": along_tp(dx)} for dx in range(1, chips)]
        + [{"grp": along_grp(dg)} for dg in range(1, n_grp)]
        + [{"tp": partner}]
    )
    for peer in peers:
        pl.semaphore_signal(barrier, inc=1, device_id=peer, device_id_type=MESH)
    spread_gain(0)
    fold(0)
    pl.semaphore_wait(barrier, len(peers))

    p_start(0)
    z_start(0, 0)
    load(3).start()
    fold(1)
    p_start(1)
    z_start(1, 0)
    spread_gain(1)
    fold(2)
    round_down(0)
    load(5).start()
    fold(3)
    round_down(1)
    prompt_copy.wait()
    stream[...] = normed[...].astype(jnp.float32)
    norm()

    own_first(0)
    own_first(1)
    relay(0)
    own_later(0)
    relay(1)
    own_later(1)

    @pl.when(crooked)
    def _():
        p_start(2)

    primary(0, True, 1, 2)
    primary(1, True, 1, 2)
    crossed(0, 0, 1)
    crossed(1, 0, 1)
    primary(0, True, 2)
    primary(1, True, 2)

    @pl.when(straight)
    def _():
        p_start(2)

    z_start(2, 0)
    crossed(0, 1)
    crossed(1, 1)
    p_start(3)
    z_start(3, 0)
    down_start(0)
    relay(2)
    complete(0, near)
    complete(1, near)
    own_first(2)
    secondary(0)
    own_later(2)
    relay(3)
    own_first(3)
    own_later(3)
    primary(2, straight)
    secondary(1)
    primary(2, crooked, 1, 2)
    complete(0, far)
    gate_part(0)
    complete(1, far)
    up_part(0)
    primary(3, straight)
    for j in range(strips):
        down_ready(0, 0, j)

    def beside(i):
        @pl.when(i == 0)
        def _():
            primary(2, crooked, 2)
            primary(3, crooked)

        @pl.when(i == 6)
        def _():
            down_start(1)

        per = -(-n_fs // 4)
        for m in (2, 3):
            for q in range(per):
                n = i // 2 * per + q

                @pl.when(jnp.logical_and(lane(m), jnp.logical_and(lax.rem(i, 2) == 1, n < n_fs)))
                def _():
                    crossed_step(m, n)

        for q in range(per):
            n = (i - 8) * per + q
            ripe = jnp.logical_and(n >= 0, n < n_fs)

            @pl.when(jnp.logical_and(lane(2), jnp.logical_and(jnp.logical_not(is_mid), ripe)))
            def _():
                secondary_step(2, n)

    reduce(0, beside)
    norm()
    secondary(2, is_mid)
    secondary(3)
    complete(2, near)
    complete(2, far)
    gate_part(1)
    complete(3, near)
    complete(3, far)
    up_part(1)
    for j in range(strips):
        down_ready(1, 0, j)
    reduce(1)

    for m in range(4):
        for s in range(columns_to[m]):
            if s > 0:
                p_copy(m, s).wait_send()
            for j in range(ratio):
                @pl.when(z_copy(m, s, j)[2] != f)
                def _():
                    z_remote(m, s, j).wait_send()

                if m % 2 == 1:
                    @pl.when(z_copy(m, s, j)[2] == f)
                    def _():
                        z_aside(m, s, j).wait_send()

        @pl.when(lane(m))
        def _():
            if not WHOLE[m]:
                @pl.when(carries)
                def _():
                    for dx in range(1, chips):
                        arrived(rows_of(m, n_fs * (share // n_sub)), x_send.at[m])

            for dg in range(1, n_grp):
                arrived(rows_of(m, n_fs * share), y_send.at[m])
            arrived(served[m], c_send.at[m])

    for k in range(2):
        for j in range(strips):
            dc_copy(k, 0, j).wait_send()
            for dx in range(1, chips):
                dx_copy(k, dx, j).wait_send()
                dc_copy(k, dx, j).wait_send()

        arrived(onward.at[k], s_send.at[k])

        @pl.when(jnp.logical_not(is_end))
        def _():
            arrived(final[k], o_send.at[k])


def store(halves, parts, *refs):
    ins, outs, sems = refs[:7], refs[7:14], refs[14]
    copies = []
    pieces, rows, wide = ins[0].shape
    for n in range(pieces):
        at = pl.ds(n % halves * rows, rows), pl.ds(n // halves * wide, wide)
        copies.append((ins[0].at[n], outs[0].at[at]))
    for src, dst in zip(ins[1:], outs[1:]):
        rows = src.shape[0] // parts
        for i in range(parts):
            at = pl.ds(i * rows, rows)
            copies.append((src.at[at], dst.at[at]))
    copies = [pltpu.make_async_copy(src, dst, sems.at[i]) for i, (src, dst) in enumerate(copies)]
    for copy in copies:
        copy.start()
    for copy in copies:
        copy.wait()


def on_device(
    n_grp, n_fs, n_tp,
    prompt,
    gain_first,
    gate_first,
    up_first,
    down_first,
    gain_second,
    gate_second,
    up_second,
    down_second,
):
    tokens, features = prompt.shape
    rows, columns = gate_first.shape
    width = columns * n_tp // n_fs
    d_rows, d_cols = down_first.shape
    chips = n_tp // 2
    wide = min(256, features)
    halves = HALVES if tokens % (16 * HALVES) == 0 else 1
    chunks = features // wide
    parts = (chunks * halves, tokens // halves, wide)
    strips = d_cols // wide
    gate_shape, down_shape = (features, width), (d_rows, features)
    bf16 = functools.partial(jax.ShapeDtypeStruct, dtype=jnp.bfloat16)
    share = rows // n_grp
    n_sub = chips if share % (16 * chips) == 0 else 1
    other_x, other_g = max(chips - 1, 1), max(n_grp - 1, 1)
    sems = [
        (6,), (2,), (),
        (4, other_x), (4, other_x), (4, other_x, n_fs // n_tp),
        (4, n_fs // n_tp), (4, n_fs), (4,), (4, n_fs, n_sub), (4,), (4, n_fs, other_g, n_sub),
        (4,), (4, n_grp), (4,),
        (2, other_x, strips), (2, other_x, strips), (2, chips, strips), (2, chips, strips),
        (2,), (2, parts[0]), (2, parts[0]), (2,),
    ]
    if rows % LANES == 0:
        gains = [gain.reshape(1, rows) for gain in (gain_first, gain_second)]
    else:
        gains = [jnp.broadcast_to(gain[:, None], (rows, LANES)) for gain in (gain_first, gain_second)]
    far = functools.partial(pltpu.with_memory_space_constraint, memory_space=pltpu.HBM)
    vmem, hbm = pl.BlockSpec(memory_space=pltpu.VMEM), pl.BlockSpec(memory_space=pltpu.HBM)
    shapes = [parts] + [gate_shape] * 4 + [down_shape] * 2
    held = pl.pallas_call(
        functools.partial(kernel, n_grp, n_fs, n_tp, n_sub),
        out_shape=[bf16(s) for s in shapes],
        in_specs=[hbm] * 9,
        out_specs=[vmem] * 7,
        scratch_shapes=[
            [pltpu.VMEM((rows, columns), jnp.float32)] * 3 + [pltpu.VMEM((d_rows, d_cols), jnp.float32)],
            pltpu.VMEM((2, *gains[0].shape), jnp.float32),
            pltpu.VMEM((4, rows, columns), jnp.bfloat16),
            pltpu.VMEM((2, rows, LANES), jnp.float32),
            pltpu.VMEM((tokens, features), jnp.float32),
            pltpu.VMEM((tokens, features), jnp.bfloat16),
            pltpu.VMEM((tokens, width), jnp.bfloat16),
            pltpu.VMEM((tokens, width), jnp.float32),
            pltpu.VMEM((2, *parts), jnp.bfloat16),
            pltpu.VMEM((2, *parts), jnp.bfloat16),
            pltpu.VMEM((2, *parts), jnp.bfloat16),
            pltpu.VMEM(parts, jnp.bfloat16),
            [
                pltpu.VMEM((other_x, share // (1 if whole else n_sub), columns), jnp.bfloat16)
                for whole in WHOLE
            ],
        ]
        + [pltpu.SemaphoreType.DMA(s) for s in sems],
        compiler_params=pltpu.CompilerParams(
            collective_id=0, has_side_effects=True, vmem_limit_bytes=27 * 2**20
        ),
        name="serve",
    )(far(prompt), *map(far, gains), *map(far, (gate_first, up_first, gate_second, up_second, down_first, down_second)))
    result, g1, u1, g2, u2, d1, d2 = pl.pallas_call(
        functools.partial(store, halves, SPLIT),
        out_shape=[bf16((tokens, features))] + [bf16(s) for s in shapes[1:]],
        in_specs=[vmem] * 7,
        out_specs=[hbm] * 7,
        scratch_shapes=[pltpu.SemaphoreType.DMA((parts[0] + 6 * SPLIT,))],
        compiler_params=pltpu.CompilerParams(vmem_limit_bytes=2**20),
        name="store",
    )(*held)
    return (result, g1, u1, d1, g2, u2, d2)
def solution(mesh):
    return jax.shard_map(
        functools.partial(on_device, mesh.shape["grp"], mesh.shape["fs"], mesh.shape["tp"]),
        mesh=mesh,
        in_specs=(
            P(("grp", "tp"), None),
            P("fs"),
            P("fs", "tp"),
            P("fs", "tp"),
            P("fs", "tp"),
            P("fs"),
            P("fs", "tp"),
            P("fs", "tp"),
            P("fs", "tp"),
        ),
        out_specs=(
            P(("grp", "tp"), None),
            P("grp", "fs"),
            P("grp", "fs"),
            P("fs", "grp"),
            P("grp", "fs"),
            P("grp", "fs"),
            P("fs", "grp"),
        ),
        check_vma=False,
    )
```

```python
import functools

import jax
import jax.numpy as jnp
from jax import lax
from jax.experimental import pallas as pl
from jax.experimental.pallas import tpu as pltpu
from jax.sharding import PartitionSpec as P

EPS = 1e-06
MESH = pl.DeviceIdType.MESH
LANES = 128
LAG = 1
LEAD = 3
HALVES = 2
SPLIT = 4
WHOLE = (False, False, False, False)


def kernel(n_grp, n_fs, n_tp, n_sub, *refs):
    prompt, gains, weights, downs = refs[0], refs[1:3], refs[3:7], refs[7:9]
    result, served, served_down = refs[9], refs[10:14], refs[14:16]
    (land, gain_land, own, scale, stream, normed, hidden, opened, onward, inward, middle, delta, stage) = refs[16:29]
    (load_sem, gain_sem, prompt_sem,
     p_send, p_recv, r_send, z_send, z_recv, x_send, x_recv, y_send, y_recv, c_send, c_recv, own_sem,
     dx_send, dx_recv, dc_send, dc_recv,
     s_send, u_recv, back, o_send) = refs[29:]

    g, f, t = lax.axis_index("grp"), lax.axis_index("fs"), lax.axis_index("tp")
    ratio = n_fs // n_tp
    chips = n_tp // 2
    home = f // ratio
    mine_sub = lax.rem(t // 2 + chips - home // 2, chips)
    carries = mine_sub < n_sub
    partner = t + 1 - 2 * lax.rem(t, 2)

    def lane(m):
        return lax.rem(t + m, 2) == lax.rem(home, 2)

    def other_lane(m):
        return lax.rem(t + m, 2) != lax.rem(home, 2)

    half = n_fs // 2
    lower = f < half
    is_mid = jnp.logical_or(f == half - 1, f == half)
    is_end = jnp.logical_or(f == 0, f == n_fs - 1)
    toward = jnp.where(lower, f + 1, f - 1)
    away = jnp.where(lower, jnp.maximum(f - 1, 0), jnp.minimum(f + 1, n_fs - 1))

    depth = jnp.where(lower, f, n_fs - 1 - f)

    def along_fs(o):
        return lax.rem(f + o, n_fs)

    def by_way(o):
        r = jnp.where(o <= depth, depth - o, o)
        return jnp.where(lower, r, n_fs - 1 - r)

    def along_tp(dx):
        return lax.rem(t + 2 * dx, n_tp)

    def along_grp(dg):
        return lax.rem(g + dg, n_grp)

    def remote(src, dst, send, recv, where):
        return pltpu.make_async_remote_copy(
            src_ref=src, dst_ref=dst, send_sem=send, recv_sem=recv,
            device_id=where, device_id_type=MESH,
        )

    def arrived(dst, sem):
        pltpu.make_async_copy(dst, dst, sem).wait()

    rows, columns = weights[0].shape
    share = rows // n_grp
    subs = [1 if whole else n_sub for whole in WHOLE]
    columns_to = [chips if whole else n_sub for whole in WHOLE]
    width = served[0].shape[1]
    d_rows, d_cols = downs[0].shape
    tokens, features = prompt.shape
    slab = min(64, tokens)
    tile = min(512, width)
    wide = min(256, features)
    chunks = features // wide
    strips = d_cols // wide
    halves, part_rows, _ = result.shape[0] // chunks, *result.shape[1:]

    def landing(n):
        return land[n % 3] if n < 4 else land[3]

    def load(n):
        src = weights[n] if n < 4 else downs[n - 4]
        return pltpu.make_async_copy(src, landing(n), load_sem.at[n])

    def gain_copy(k):
        return pltpu.make_async_copy(gains[k], gain_land.at[k], gain_sem.at[k])

    def spread_gain(k):
        gain_copy(k).wait()
        gain = gain_land.at[k]
        if gain.shape[0] == rows:
            scale[k] = gain[...]
        else:
            scale[k] = jnp.broadcast_to(gain[...], (LANES, rows)).T

    def fold(m):
        load(m).wait()
        step = min(64, rows)

        @pl.loop(0, rows // step)
        def _(i):
            at = pl.ds(pl.multiple_of(i * step, step), step)
            factor = scale[m // 2, at]
            for j in range(columns // LANES):
                lanes = pl.ds(j * LANES, LANES)
                own[m, at, lanes] = (factor * landing(m)[at, lanes]).astype(jnp.bfloat16)

    def round_down(k):
        load(4 + k).wait()
        step = min(64, d_rows)

        @pl.loop(0, d_rows // step)
        def _(i):
            at = pl.ds(pl.multiple_of(i * step, step), step)
            to = pl.ds(pl.multiple_of(t * d_cols, d_cols), d_cols)
            served_down[k][at, to] = landing(4 + k)[at].astype(jnp.bfloat16)

    def carried(m, s):
        return 0 if WHOLE[m] else s

    def piece(m, r, h, s):
        sub = share // subs[m]
        return served[m].at[pl.ds(pl.multiple_of(r * rows + h * share + s * sub, sub), sub)]

    def rows_of(m, count):
        return served[m].at[pl.ds(0, count)]

    def own_rows(m, s):
        sub = share // subs[m]
        return pl.ds(pl.multiple_of(g * share + carried(m, s) * sub, sub), sub)

    def p_copy(m, s):
        src = own.at[m, own_rows(m, s)]
        return remote(src, stage[m].at[s - 1], p_send.at[m, s - 1], p_recv.at[m, s - 1], {"tp": along_tp(s)})

    def p_start(m):
        for s in range(1, columns_to[m]):
            p_copy(m, s).start()

    def z_copy(m, s, j):
        cut = pl.ds(j * width, width)
        if s == 0:
            return own.at[m, own_rows(m, 0), cut], piece(m, f, g, 0), t * ratio + j
        source = lax.rem(t + n_tp - 2 * s, n_tp)
        return stage[m].at[s - 1, :, cut], piece(m, f, g, carried(m, s)), source * ratio + j

    def z_remote(m, s, j):
        src, dst, to = z_copy(m, s, j)
        send = z_send.at[m, j] if s == 0 else r_send.at[m, s - 1, j]
        where = {"fs": to} if m % 2 == 0 else {"fs": to, "tp": partner}
        return remote(src, dst, send, z_recv.at[m, f], where)

    def z_aside(m, s, j):
        src, dst, _ = z_copy(m, s, j)
        send = z_send.at[m, j] if s == 0 else r_send.at[m, s - 1, j]
        return remote(src, dst, send, own_sem.at[m], {"tp": partner})

    def z_start(m, s):
        for j in range(ratio):
            src, dst, to = z_copy(m, s, j)

            @pl.when(to != f)
            def _():
                z_remote(m, s, j).start()

            @pl.when(to == f)
            def _():
                if m % 2 == 0:
                    pltpu.make_async_copy(src, dst, own_sem.at[m]).start()
                else:
                    z_aside(m, s, j).start()

    def relay(m):
        for s in range(1, columns_to[m]):
            arrived(stage[m].at[s - 1], p_recv.at[m, s - 1])
            z_start(m, s)

    def x_copy(m, r, dx):
        ref = piece(m, r, g, mine_sub)
        return remote(ref, ref, x_send.at[m], x_recv.at[m, r, mine_sub], {"tp": along_tp(dx)})

    def y_copy(m, r, dg, s):
        ref = piece(m, r, g, s)
        return remote(ref, ref, y_send.at[m], y_recv.at[m, r, dg - 1, s], {"grp": along_grp(dg)})

    def c_copy(m, r, h, s):
        ref = piece(m, r, h, s)
        return remote(ref, ref, c_send.at[m], c_recv.at[m, h], {"tp": partner})

    def primary_step(m, o):
        r = by_way(o)
        s = 0 if WHOLE[m] else mine_sub
        ref = piece(m, r, g, s)

        def onward_from(first):
            arrived(ref, own_sem.at[m] if first else z_recv.at[m, r])
            if not WHOLE[m]:
                for dx in range(1, chips):
                    x_copy(m, r, dx).start()
            for dg in range(1, n_grp):
                y_copy(m, r, dg, s).start()
            c_copy(m, r, g, s).start()

        if WHOLE[m]:
            onward_from(isinstance(o, int))
        else:
            @pl.when(carries)
            def _():
                onward_from(isinstance(o, int))

    def own_first(m):
        @pl.when(jnp.logical_and(lane(m), mine_sub == 0))
        def _():
            primary_step(m, 0)

    def own_later(m):
        @pl.when(jnp.logical_and(lane(m), mine_sub != 0))
        def _():
            primary_step(m, 0)

    straight = mine_sub == 0
    crooked = mine_sub != 0

    def primary(m, where=True, low=1, high=n_fs):
        @pl.when(jnp.logical_and(lane(m), where))
        def _():
            @pl.loop(low, high)
            def _(o):
                primary_step(m, o)

    def crossed_step(m, o):
        r = by_way(o)
        for s in range(0 if WHOLE[m] else n_sub):
            @pl.when(mine_sub != s)
            def _():
                arrived(piece(m, r, g, s), x_recv.at[m, r, s])
                for dg in range(1, n_grp):
                    y_copy(m, r, dg, s).start()
                c_copy(m, r, g, s).start()

    def crossed(m, low=0, high=n_fs):
        @pl.when(lane(m))
        def _():
            @pl.loop(low, high)
            def _(o):
                crossed_step(m, o)

    def secondary_step(m, o):
        r = by_way(o)
        for dg in range(1, n_grp):
            h = along_grp(dg)
            for s in range(subs[m]):
                arrived(piece(m, r, h, s), y_recv.at[m, r, n_grp - dg - 1, s])
                c_copy(m, r, h, s).start()

    def secondary(m, where=True):
        @pl.when(jnp.logical_and(lane(m), where))
        def _():
            @pl.loop(0, n_fs)
            def _(o):
                secondary_step(m, o)

    def complete(m, groups):
        @pl.when(other_lane(m))
        def _():
            for dg in groups:
                arrived(rows_of(m, n_fs * share), c_recv.at[m, along_grp(dg)])

    near, far = range(1), range(1, n_grp)

    def d_strip(k, s, j):
        return served_down[k].at[:, pl.ds(pl.multiple_of(s * d_cols + j * wide, wide), wide)]

    def d_from(device, dx):
        return lax.rem(device + n_tp - 2 * dx, n_tp)

    def dx_copy(k, dx, j):
        ref = d_strip(k, t, j)
        return remote(ref, ref, dx_send.at[k, dx - 1, j], dx_recv.at[k, dx - 1, j], {"tp": along_tp(dx)})

    def dc_copy(k, dx, j):
        ref = d_strip(k, d_from(t, dx), j)
        return remote(ref, ref, dc_send.at[k, dx, j], dc_recv.at[k, dx, j], {"tp": partner})

    def down_start(k):
        for j in range(strips):
            for dx in range(1, chips):
                dx_copy(k, dx, j).start()
            dc_copy(k, 0, j).start()

    def down_pass(k, dx, j):
        arrived(d_strip(k, d_from(t, dx), j), dx_recv.at[k, dx - 1, j])
        dc_copy(k, dx, j).start()

    def down_ready(k, dx, j):
        arrived(d_strip(k, d_from(partner, dx), j), dc_recv.at[k, dx, j])

    final = (delta, result)

    def to_middle(k, i):
        return remote(onward.at[k, i], middle.at[k, i], s_send.at[k], back.at[k, i], {"fs": toward})

    def to_next(k, i):
        return remote(onward.at[k, i], inward.at[k, i], s_send.at[k], u_recv.at[k, i], {"fs": toward})

    def to_outer(k, i):
        ref = final[k].at[i]
        return remote(ref, ref, o_send.at[k], back.at[k, i], {"fs": away})

    def place(n):
        i, h = n // halves, lax.rem(n, halves)
        return (
            pl.ds(pl.multiple_of(h * part_rows, part_rows), part_rows),
            pl.ds(pl.multiple_of(i * wide, wide), wide),
        )

    def gather_in(k, i):
        at = pl.ds(pl.multiple_of(i * wide, wide), wide)
        value = jnp.dot(hidden[...], served_down[k][:, at], preferred_element_type=jnp.float32)
        for h in range(halves):
            n = i * halves + h
            own_part = value[h * part_rows : (h + 1) * part_rows]

            @pl.when(is_end)
            def _():
                onward[k, n] = own_part.astype(jnp.bfloat16)

            @pl.when(jnp.logical_not(is_end))
            def _():
                arrived(inward.at[k, n], u_recv.at[k, n])
                onward[k, n] = (own_part + inward[k, n].astype(jnp.float32)).astype(jnp.bfloat16)

            @pl.when(is_mid)
            def _():
                to_middle(k, n).start()

            @pl.when(jnp.logical_not(is_mid))
            def _():
                to_next(k, n).start()

    def spread_out(k, n):
        at = place(n)

        @pl.when(is_mid)
        def _():
            arrived(middle.at[k, n], back.at[k, n])
            total = 0.5 * (onward[k, n].astype(jnp.float32) + middle[k, n].astype(jnp.float32))
            if k == 1:
                total = stream[at] + total
            final[k][n] = total.astype(jnp.bfloat16)

        @pl.when(jnp.logical_not(is_mid))
        def _():
            arrived(final[k].at[n], back.at[k, n])

        @pl.when(jnp.logical_not(is_end))
        def _():
            to_outer(k, n).start()

        if k == 0:
            stream[at] = stream[at] + delta[n].astype(jnp.float32)

    per_chip = chunks // chips

    def chunk_of(i):
        chip = lax.rem(t // 2 + chips - i // per_chip, chips)
        j = lax.rem(i, per_chip)
        return chip * per_chip + lax.rem(j, 2) * strips + j // 2

    def reduce(k, beside=None):
        lag = jnp.where(is_mid, LAG, chunks)
        first = jnp.where(is_end, LEAD, 1)

        @pl.loop(0, jnp.where(is_mid, chunks + LAG, 2 * chunks))
        def _(i):
            if beside is not None:
                @pl.when(i >= first)
                def _():
                    beside(i - first)

            @pl.when(i < chunks)
            def _():
                for dx in range(1, chips):
                    for j in range(strips):
                        @pl.when(i == dx * per_chip + 2 * j - 1)
                        def _():
                            down_pass(k, dx, j)

                        @pl.when(i == dx * per_chip + 2 * j)
                        def _():
                            down_ready(k, dx, j)

                gather_in(k, chunk_of(i))

            @pl.when(i >= lag)
            def _():
                for h in range(halves):
                    spread_out(k, chunk_of(i - lag) * halves + h)

    def norm():
        @pl.loop(0, tokens // slab)
        def _(i):
            at = pl.ds(pl.multiple_of(i * slab, slab), slab)
            value = stream[at]
            factor = lax.rsqrt(jnp.mean(value * value, axis=-1, keepdims=True) + EPS)
            normed[at] = (value * factor).astype(jnp.bfloat16)

    def gate_part(k):
        @pl.loop(0, width // tile)
        def _(i):
            at = pl.ds(pl.multiple_of(i * tile, tile), tile)
            gate = jnp.dot(normed[...], served[2 * k][:, at], preferred_element_type=jnp.float32)
            opened[:, at] = jax.nn.silu(gate)

    def up_part(k):
        @pl.loop(0, width // tile)
        def _(i):
            at = pl.ds(pl.multiple_of(i * tile, tile), tile)
            up = jnp.dot(normed[...], served[2 * k + 1][:, at], preferred_element_type=jnp.float32)
            hidden[:, at] = (opened[:, at] * up).astype(jnp.bfloat16)

    gain_copy(0).start()
    for n in (0, 1, 2, 4):
        load(n).start()
    gain_copy(1).start()
    prompt_copy = pltpu.make_async_copy(prompt, normed, prompt_sem)
    prompt_copy.start()

    barrier = pltpu.get_barrier_semaphore()
    peers = (
        [{"fs": along_fs(o)} for o in range(1, n_fs)]
        + [{"fs": along_fs(o), "tp": partner} for o in range(1, n_fs)]
        + [{"tp": along_tp(dx)} for dx in range(1, chips)]
        + [{"grp": along_grp(dg)} for dg in range(1, n_grp)]
        + [{"tp": partner}]
    )
    for peer in peers:
        pl.semaphore_signal(barrier, inc=1, device_id=peer, device_id_type=MESH)
    spread_gain(0)
    fold(0)
    pl.semaphore_wait(barrier, len(peers))

    p_start(0)
    z_start(0, 0)
    load(3).start()
    fold(1)
    p_start(1)
    z_start(1, 0)
    spread_gain(1)
    fold(2)
    round_down(0)
    load(5).start()
    fold(3)
    round_down(1)
    prompt_copy.wait()
    stream[...] = normed[...].astype(jnp.float32)
    norm()

    own_first(0)
    own_first(1)
    relay(0)
    own_later(0)
    relay(1)
    own_later(1)

    @pl.when(crooked)
    def _():
        p_start(2)

    primary(0, True, 1, 2)
    primary(1, True, 1, 2)
    crossed(0, 0, 1)
    crossed(1, 0, 1)
    primary(0, True, 2)
    primary(1, True, 2)

    @pl.when(straight)
    def _():
        p_start(2)

    z_start(2, 0)
    crossed(0, 1)
    crossed(1, 1)
    p_start(3)
    z_start(3, 0)
    down_start(0)
    relay(2)
    complete(0, near)
    complete(1, near)
    own_first(2)
    secondary(0)
    own_later(2)
    relay(3)
    own_first(3)
    own_later(3)
    primary(2, straight)
    secondary(1)
    primary(2, crooked)
    complete(0, far)
    gate_part(0)
    complete(1, far)
    up_part(0)
    primary(3, straight)
    for j in range(strips):
        down_ready(0, 0, j)

    def beside(i):
        @pl.when(i == 0)
        def _():
            primary(3, crooked)

        @pl.when(i == 6)
        def _():
            down_start(1)

        per = -(-n_fs // 4)
        for m in (2, 3):
            for q in range(per):
                n = i // 2 * per + q

                @pl.when(jnp.logical_and(lane(m), jnp.logical_and(lax.rem(i, 2) == 1, n < n_fs)))
                def _():
                    crossed_step(m, n)

        for q in range(per):
            n = (i - 8) * per + q
            ripe = jnp.logical_and(n >= 0, n < n_fs)

            @pl.when(jnp.logical_and(lane(2), jnp.logical_and(jnp.logical_not(is_mid), ripe)))
            def _():
                secondary_step(2, n)

    reduce(0, beside)
    norm()
    secondary(2, is_mid)
    secondary(3)
    complete(2, near)
    complete(2, far)
    gate_part(1)
    complete(3, near)
    complete(3, far)
    up_part(1)
    for j in range(strips):
        down_ready(1, 0, j)
    reduce(1)

    for m in range(4):
        for s in range(columns_to[m]):
            if s > 0:
                p_copy(m, s).wait_send()
            for j in range(ratio):
                @pl.when(z_copy(m, s, j)[2] != f)
                def _():
                    z_remote(m, s, j).wait_send()

                if m % 2 == 1:
                    @pl.when(z_copy(m, s, j)[2] == f)
                    def _():
                        z_aside(m, s, j).wait_send()

        @pl.when(lane(m))
        def _():
            if not WHOLE[m]:
                @pl.when(carries)
                def _():
                    for dx in range(1, chips):
                        arrived(rows_of(m, n_fs * (share // n_sub)), x_send.at[m])

            for dg in range(1, n_grp):
                arrived(rows_of(m, n_fs * share), y_send.at[m])
            arrived(served[m], c_send.at[m])

    for k in range(2):
        for j in range(strips):
            dc_copy(k, 0, j).wait_send()
            for dx in range(1, chips):
                dx_copy(k, dx, j).wait_send()
                dc_copy(k, dx, j).wait_send()

        arrived(onward.at[k], s_send.at[k])

        @pl.when(jnp.logical_not(is_end))
        def _():
            arrived(final[k], o_send.at[k])


def store(halves, parts, *refs):
    ins, outs, sems = refs[:7], refs[7:14], refs[14]
    copies = []
    pieces, rows, wide = ins[0].shape
    for n in range(pieces):
        at = pl.ds(n % halves * rows, rows), pl.ds(n // halves * wide, wide)
        copies.append((ins[0].at[n], outs[0].at[at]))
    for src, dst in zip(ins[1:], outs[1:]):
        rows = src.shape[0] // parts
        for i in range(parts):
            at = pl.ds(i * rows, rows)
            copies.append((src.at[at], dst.at[at]))
    copies = [pltpu.make_async_copy(src, dst, sems.at[i]) for i, (src, dst) in enumerate(copies)]
    for copy in copies:
        copy.start()
    for copy in copies:
        copy.wait()


def on_device(
    n_grp, n_fs, n_tp,
    prompt,
    gain_first,
    gate_first,
    up_first,
    down_first,
    gain_second,
    gate_second,
    up_second,
    down_second,
):
    tokens, features = prompt.shape
    rows, columns = gate_first.shape
    width = columns * n_tp // n_fs
    d_rows, d_cols = down_first.shape
    chips = n_tp // 2
    wide = min(256, features)
    halves = HALVES if tokens % (16 * HALVES) == 0 else 1
    chunks = features // wide
    parts = (chunks * halves, tokens // halves, wide)
    strips = d_cols // wide
    gate_shape, down_shape = (features, width), (d_rows, features)
    bf16 = functools.partial(jax.ShapeDtypeStruct, dtype=jnp.bfloat16)
    share = rows // n_grp
    n_sub = chips if share % (16 * chips) == 0 else 1
    other_x, other_g = max(chips - 1, 1), max(n_grp - 1, 1)
    sems = [
        (6,), (2,), (),
        (4, other_x), (4, other_x), (4, other_x, n_fs // n_tp),
        (4, n_fs // n_tp), (4, n_fs), (4,), (4, n_fs, n_sub), (4,), (4, n_fs, other_g, n_sub),
        (4,), (4, n_grp), (4,),
        (2, other_x, strips), (2, other_x, strips), (2, chips, strips), (2, chips, strips),
        (2,), (2, parts[0]), (2, parts[0]), (2,),
    ]
    if rows % LANES == 0:
        gains = [gain.reshape(1, rows) for gain in (gain_first, gain_second)]
    else:
        gains = [jnp.broadcast_to(gain[:, None], (rows, LANES)) for gain in (gain_first, gain_second)]
    far = functools.partial(pltpu.with_memory_space_constraint, memory_space=pltpu.HBM)
    vmem, hbm = pl.BlockSpec(memory_space=pltpu.VMEM), pl.BlockSpec(memory_space=pltpu.HBM)
    shapes = [parts] + [gate_shape] * 4 + [down_shape] * 2
    held = pl.pallas_call(
        functools.partial(kernel, n_grp, n_fs, n_tp, n_sub),
        out_shape=[bf16(s) for s in shapes],
        in_specs=[hbm] * 9,
        out_specs=[vmem] * 7,
        scratch_shapes=[
            [pltpu.VMEM((rows, columns), jnp.float32)] * 3 + [pltpu.VMEM((d_rows, d_cols), jnp.float32)],
            pltpu.VMEM((2, *gains[0].shape), jnp.float32),
            pltpu.VMEM((4, rows, columns), jnp.bfloat16),
            pltpu.VMEM((2, rows, LANES), jnp.float32),
            pltpu.VMEM((tokens, features), jnp.float32),
            pltpu.VMEM((tokens, features), jnp.bfloat16),
            pltpu.VMEM((tokens, width), jnp.bfloat16),
            pltpu.VMEM((tokens, width), jnp.float32),
            pltpu.VMEM((2, *parts), jnp.bfloat16),
            pltpu.VMEM((2, *parts), jnp.bfloat16),
            pltpu.VMEM((2, *parts), jnp.bfloat16),
            pltpu.VMEM(parts, jnp.bfloat16),
            [
                pltpu.VMEM((other_x, share // (1 if whole else n_sub), columns), jnp.bfloat16)
                for whole in WHOLE
            ],
        ]
        + [pltpu.SemaphoreType.DMA(s) for s in sems],
        compiler_params=pltpu.CompilerParams(
            collective_id=0, has_side_effects=True, vmem_limit_bytes=27 * 2**20
        ),
        name="serve",
    )(far(prompt), *map(far, gains), *map(far, (gate_first, up_first, gate_second, up_second, down_first, down_second)))
    result, g1, u1, g2, u2, d1, d2 = pl.pallas_call(
        functools.partial(store, halves, SPLIT),
        out_shape=[bf16((tokens, features))] + [bf16(s) for s in shapes[1:]],
        in_specs=[vmem] * 7,
        out_specs=[hbm] * 7,
        scratch_shapes=[pltpu.SemaphoreType.DMA((parts[0] + 6 * SPLIT,))],
        compiler_params=pltpu.CompilerParams(vmem_limit_bytes=2**20),
        name="store",
    )(*held)
    return (result, g1, u1, d1, g2, u2, d2)
def solution(mesh):
    return jax.shard_map(
        functools.partial(on_device, mesh.shape["grp"], mesh.shape["fs"], mesh.shape["tp"]),
        mesh=mesh,
        in_specs=(
            P(("grp", "tp"), None),
            P("fs"),
            P("fs", "tp"),
            P("fs", "tp"),
            P("fs", "tp"),
            P("fs"),
            P("fs", "tp"),
            P("fs", "tp"),
            P("fs", "tp"),
        ),
        out_specs=(
            P(("grp", "tp"), None),
            P("grp", "fs"),
            P("grp", "fs"),
            P("fs", "grp"),
            P("grp", "fs"),
            P("grp", "fs"),
            P("fs", "grp"),
        ),
        check_vma=False,
    )
```
